256 devices in a mesh: grp: 2 (over y), sp: 16 (over z), tp: 8 (over x, core).
Axes of the slice: x: 4, y: 2, z: 16, core: 2. Of those that a mesh axis runs over, the one named last changes fastest.
The devices are a block of a 4x16x16 slice.
Arguments:
- queries: bfloat16 [24576, 1024], P(('grp', 'sp'), 'tp'), parts along dimension 0, may hold values from -200 to 200
- key_rows: bfloat16 [24576, 512], P(('grp', 'sp'), 'tp'), parts along dimension 0, may hold values from -6 to 6
- value_rows: bfloat16 [24576, 512], P(('grp', 'sp'), 'tp'), parts along dimension 0, may hold values from -6 to 6
- doc_ids: int32 [24576], P(('grp', 'sp')), parts along dimension 0, may hold values from 0 to 7, never falling along the last dimension, each value on 1 to 3072 neighbouring positions
- sink_logits: float32 [16], P('tp'), may hold values from 2 to 7
- out_weight: bfloat16 [1024, 2048], P('tp', 'sp'), may hold values from -0.1875 to 0.1875
- residual: bfloat16 [24576, 2048], P(('grp', 'sp', 'tp')), parts along dimension 0, may hold values from -6 to 6
- gain_mixed: float32 [2048], replicated, may hold values from 0.1 to 1.9
- gain_before: float32 [2048], replicated, may hold values from 0.1 to 1.9
- gain_after: float32 [2048], replicated, may hold values from 0.1 to 1.9
- gate_weight: bfloat16 [2048, 6144], P('sp', 'tp'), may hold values from -0.125 to 0.125
- up_weight: bfloat16 [2048, 6144], P('sp', 'tp'), may hold values from -0.125 to 0.125
- down_weight: bfloat16 [6144, 2048], P('tp', 'sp'), may hold values from -0.078125 to 0.078125
Outputs:
- layer_out: bfloat16 [24576, 2048], P(('grp', 'sp', 'tp')), parts along dimension 0
The draws below stay inside these ranges and needn't reach their ends.
There are 2 independent parts, one for each index of `grp`. The reference program is written for one: setup_inputs(seed, part) draws one part's arguments, and reference() takes and returns one part's arrays. A program takes and returns all parts, laid end to end along the dimension named above; an argument that names none is the same for every part. Nothing has to cross between parts.
All inputs are finite; a program needn't handle non-finite values.
Results may differ from the reference program's by a relative error of at most 0.015.
Values may be sent and summed in bfloat16 or wider, within the bound.
A program may use at most 128 MiB of HBM per device.

```python
import math
import jax
import jax.numpy as jnp
import numpy as np
from jax import lax

D = 2048
HEADS = 16
KV_HEADS = 8
HEAD_DIM = 64
FF = 6144
WINDOW = 128
TOKENS = 12288
DOCS = 8
DOC_MOST = 3072
N_TP = 8


def drawn(key):
    base_keys = jnp.clip(jax.random.normal(jax.random.fold_in(key, 11), (TOKENS, KV_HEADS * HEAD_DIM), jnp.float32), -5.0, 5.0)
    base_queries = jnp.clip(jax.random.normal(jax.random.fold_in(key, 12), (TOKENS, HEADS * HEAD_DIM), jnp.float32), -5.0, 5.0)
    return (base_queries, base_keys)


def draw_queries(key, part):
    return drawn(key)[0].astype(jnp.bfloat16)


def draw_key_rows(key, part):
    return drawn(key)[1].astype(jnp.bfloat16)


def shard_levels(key, dims, pieces, smallest, top_value):
    level, own = 1.0, jax.random.fold_in(key, 6)
    for axis_at, blocks in pieces:
        heights = jnp.exp(jax.random.uniform(jax.random.fold_in(own, axis_at), (blocks,), jnp.float32, smallest / len(pieces), top_value / len(pieces)))
        level = level * jnp.repeat(heights, dims[axis_at] // blocks).reshape([-1 if axis == axis_at else 1 for axis in range(len(dims))])
    return level


def length_profile(amount, total, bound, skew):
    weights = [(1 << 20) // math.isqrt(rank ** skew) + 1 for rank in range(2, amount + 1)]
    spare, holding = total - bound - (amount - 1), [1] * (amount - 1)
    while spare > 0:
        candidates = [i for i in range(amount - 1) if holding[i] < bound]
        mass, remaining = sum([weights[i] for i in candidates]), spare
        for i in candidates:
            more = min(bound - holding[i], max(1, remaining * weights[i] // mass), spare)
            holding[i] = holding[i] + more
            spare = spare - more
    return np.array([bound] + holding)


def uneven_parts(stream_key, count, total, bound, skew):
    if count == 2:
        one = jax.random.randint(stream_key, (), max(1, total - bound), min(bound, total - 1) + 1)
        return jnp.stack([one, total - one])
    lengths = jnp.asarray(length_profile(count, total, bound, skew), jnp.int32)
    twos = (count - 1) // 2
    source_of, taker = lengths[1:1 + 2 * twos:2], lengths[2:2 + 2 * twos:2]
    margin = jnp.minimum(source_of - 1, bound - taker)
    moved = jax.random.randint(jax.random.fold_in(stream_key, 1), (twos,), 0, 1 << 20) % (margin + 1)
    lengths = lengths.at[1:1 + 2 * twos:2].set(source_of - moved).at[2:2 + 2 * twos:2].set(taker + moved)
    return lengths[jax.random.permutation(jax.random.fold_in(stream_key, 2), count)]


def centred(stream_key, dims, width, most, split=(), kind=jnp.bfloat16):
    level = shard_levels(stream_key, dims, split, -0.22, 0.18) if split else 1.0
    drawn = jax.random.normal(stream_key, dims, jnp.float32) * width * level
    return jnp.minimum(jnp.maximum(drawn, -most), most).astype(kind)


def setup_inputs(seed: int = 0, part: int = 0) -> dict:
    arg_keys = jax.random.split(jax.random.key(seed), 14)
    own_keys = jax.random.split(jax.random.fold_in(arg_keys[13], part), 14)
    return {
        "queries": draw_queries(jax.random.fold_in(jax.random.fold_in(arg_keys[13], part), 71), part),
        "key_rows": draw_key_rows(jax.random.fold_in(jax.random.fold_in(arg_keys[13], part), 71), part),
        "value_rows": centred(own_keys[2], (TOKENS, KV_HEADS * HEAD_DIM), 1.0, 6.0, ((0, 16), (1, 8))),
        "doc_ids": jnp.searchsorted(jnp.cumsum(uneven_parts(own_keys[3], DOCS, TOKENS, DOC_MOST, 1)), jnp.arange(TOKENS), side="right").astype(jnp.int32),
        "sink_logits": jnp.clip(2.0 + 5.0 * jax.random.uniform(arg_keys[4], (HEADS,), jnp.float32) ** shard_levels(arg_keys[4], (HEADS,), ((0, 8),), -0.2, 0.2), 2.0, 7.0),
        "out_weight": centred(arg_keys[5], (HEADS * HEAD_DIM, D), (HEADS * HEAD_DIM) ** -0.5, 0.1875, ((0, 8), (1, 16))),
        "residual": centred(own_keys[6], (TOKENS, D), 1.0, 6.0, ((0, 128),)),
        "gain_mixed": jnp.clip(1.0 + 0.18 * jax.random.normal(arg_keys[7], (D,), jnp.float32), 0.1, 1.9),
        "gain_before": jnp.clip(1.0 + 0.18 * jax.random.normal(arg_keys[8], (D,), jnp.float32), 0.1, 1.9),
        "gain_after": jnp.clip(1.0 + 0.18 * jax.random.normal(arg_keys[9], (D,), jnp.float32), 0.1, 1.9),
        "gate_weight": centred(arg_keys[10], (D, FF), D ** -0.5, 0.125, ((0, 16), (1, 8))),
        "up_weight": centred(arg_keys[11], (D, FF), D ** -0.5, 0.125, ((0, 16), (1, 8))),
        "down_weight": centred(arg_keys[12], (FF, D), FF ** -0.5, 0.078125, ((0, 8), (1, 16))),
    }


epsilon = 1e-06
masked_value = -1e+30

def stored(value):
    return lax.optimization_barrier(value.astype(jnp.bfloat16)).astype(jnp.float32)

def rms_scaled(value, gain):
    return value * lax.rsqrt(lax.optimization_barrier(jnp.mean(value * value, axis=-1, keepdims=True)) + epsilon) * gain

def reference(queries, key_rows, value_rows, doc_ids, sink_logits, out_weight, residual, gain_mixed, gain_before, gain_after, gate_weight, up_weight, down_weight):
    total = queries.shape[0]
    blocks = total // WINDOW
    group_size = HEADS // KV_HEADS
    padded_keys = jnp.concatenate([jnp.zeros((WINDOW, KV_HEADS * HEAD_DIM), jnp.bfloat16), key_rows], axis=0)
    padded_values = jnp.concatenate([jnp.zeros((WINDOW, KV_HEADS * HEAD_DIM), jnp.bfloat16), value_rows], axis=0)
    padded_docs = jnp.concatenate([jnp.zeros((WINDOW,), jnp.int32) - 1, doc_ids], axis=0)
    key_pos = jnp.arange(total + WINDOW, dtype=jnp.int32) - WINDOW

    def windows(array):
        first = array[:-WINDOW].reshape((blocks, WINDOW) + array.shape[1:])
        second = array[WINDOW:].reshape((blocks, WINDOW) + array.shape[1:])
        return jnp.concatenate([first, second], axis=1)
    key_blocks = windows(padded_keys).reshape(blocks, 2 * WINDOW, KV_HEADS, HEAD_DIM).astype(jnp.float32)
    value_blocks = windows(padded_values).reshape(blocks, 2 * WINDOW, KV_HEADS, HEAD_DIM).astype(jnp.float32)
    key_docs = windows(padded_docs)
    key_places = windows(key_pos)
    query_blocks = queries.reshape(blocks, WINDOW, KV_HEADS, group_size, HEAD_DIM).astype(jnp.float32)
    query_places = jnp.arange(total, dtype=jnp.int32).reshape(blocks, WINDOW)
    query_docs = doc_ids.reshape(blocks, WINDOW)
    scores = jnp.einsum('bqhgd,bkhd->bhgqk', query_blocks, key_blocks) * HEAD_DIM ** (-0.5)
    distance = query_places[:, :, None] - key_places[:, None, :]
    valid = (distance >= 0) & (distance < WINDOW) & (key_places[:, None, :] >= 0)
    valid = valid & (query_docs[:, :, None] == key_docs[:, None, :])
    scores = jnp.where(valid[:, None, None], scores, masked_value)
    sinks = sink_logits.reshape(KV_HEADS, group_size)[None, :, :, None]
    top = jnp.maximum(lax.optimization_barrier(jnp.max(scores, axis=-1)), sinks)
    weight = jnp.exp(scores - top[..., None])
    denom = lax.optimization_barrier(jnp.sum(weight, axis=-1)) + jnp.exp(sinks - top)
    weight_b = weight.astype(jnp.bfloat16).astype(jnp.float32)
    summed = jnp.einsum('bhgqk,bkhd->bqhgd', weight_b, value_blocks)
    scale = jnp.transpose(denom, (0, 3, 1, 2))[..., None]
    mixed = (summed / scale).reshape(total, HEADS * HEAD_DIM).astype(jnp.bfloat16)
    projected = stored(jnp.dot(mixed, out_weight, preferred_element_type=jnp.float32))
    after = stored(residual.astype(jnp.float32) + rms_scaled(projected, gain_mixed))
    normed = rms_scaled(after, gain_before).astype(jnp.bfloat16)
    gate = jnp.dot(normed, gate_weight, preferred_element_type=jnp.float32)
    upward = jnp.dot(normed, up_weight, preferred_element_type=jnp.float32)
    hidden = (jax.nn.silu(gate) * upward).astype(jnp.bfloat16)
    block_size = FF // N_TP
    summed_out = jnp.zeros((total, D), jnp.float32)
    for index in range(N_TP):
        partial_sum = jnp.dot(hidden[:, index * block_size:(index + 1) * block_size], down_weight[index * block_size:(index + 1) * block_size], preferred_element_type=jnp.float32)
        summed_out = summed_out + stored(partial_sum)
    ffn_out = stored(summed_out)
    return (after + 0.5 * rms_scaled(ffn_out, gain_after)).astype(jnp.bfloat16)
```

```python
import functools

import jax
import jax.numpy as jnp
from jax import lax
from jax.experimental import pallas as pl
from jax.experimental.pallas import tpu as pltpu
from jax.sharding import PartitionSpec as P

HEAD_DIM = 64
WINDOW = 128
epsilon = 1e-06
masked_value = -1e30
MESH = pl.DeviceIdType.MESH
f32 = jnp.float32
bf16 = jnp.bfloat16

HALVES = 2


def passed_along(value, axis, steps):
    count = lax.axis_size(axis)
    first, last = (max(0, -steps), min(count, count - steps))
    return lax.ppermute(value, axis, [(source, source + steps) for source in range(first, last)])


def stored(value):
    return lax.optimization_barrier(value.astype(jnp.bfloat16)).astype(jnp.float32)


def rms_scaled(value, gain):
    return value * lax.rsqrt(jnp.mean(value * value, axis=-1, keepdims=True) + epsilon) * gain


def windows(array, blocks):
    first = array[:-WINDOW].reshape((blocks, WINDOW) + array.shape[1:])
    second = array[WINDOW:].reshape((blocks, WINDOW) + array.shape[1:])
    return jnp.concatenate([first, second], axis=1)


def attend(queries, key_rows, value_rows, doc_ids, sink_logits):
    length = queries.shape[0]
    blocks = length // WINDOW
    local_kv = key_rows.shape[1] // HEAD_DIM
    group_size = queries.shape[1] // HEAD_DIM // local_kv
    offset = lax.axis_index("sp") * length
    tail_keys, tail_values, tail_docs = passed_along(
        (key_rows[length - WINDOW :], value_rows[length - WINDOW :], doc_ids[length - WINDOW :]),
        "sp",
        1,
    )
    key_blocks = windows(jnp.concatenate([tail_keys, key_rows], axis=0), blocks).reshape(
        blocks, 2 * WINDOW, local_kv, HEAD_DIM
    )
    value_blocks = windows(jnp.concatenate([tail_values, value_rows], axis=0), blocks).reshape(
        blocks, 2 * WINDOW, local_kv, HEAD_DIM
    )
    key_docs = windows(jnp.concatenate([tail_docs, doc_ids], axis=0), blocks)
    key_places = windows(offset - WINDOW + jnp.arange(length + WINDOW, dtype=jnp.int32), blocks)
    query_places = (offset + jnp.arange(length, dtype=jnp.int32)).reshape(blocks, WINDOW)
    query_docs = doc_ids.reshape(blocks, WINDOW)
    query_blocks = queries.reshape(blocks, WINDOW, local_kv, group_size, HEAD_DIM)
    scores = jnp.einsum(
        "bqhgd,bkhd->bhgqk", query_blocks, key_blocks, preferred_element_type=jnp.float32
    ) * HEAD_DIM ** (-0.5)
    distance = query_places[:, :, None] - key_places[:, None, :]
    valid = (distance >= 0) & (distance < WINDOW) & (key_places[:, None, :] >= 0)
    valid = valid & (query_docs[:, :, None] == key_docs[:, None, :])
    scores = jnp.where(valid[:, None, None], scores, masked_value)
    sinks = sink_logits.reshape(local_kv, group_size)[None, :, :, None]
    top = jnp.maximum(jnp.max(scores, axis=-1), sinks)
    weight = jnp.exp(scores - top[..., None])
    denom = jnp.sum(weight, axis=-1) + jnp.exp(sinks - top)
    summed = jnp.einsum(
        "bhgqk,bkhd->bqhgd",
        weight.astype(jnp.bfloat16),
        value_blocks,
        preferred_element_type=jnp.float32,
    )
    scale = jnp.transpose(denom, (0, 3, 1, 2))[..., None]
    return (summed / scale).reshape(length, queries.shape[1]).astype(jnp.bfloat16)


def kernel(
    normed_ref,
    after_ref,
    gate_ref,
    up_ref,
    down_ref,
    gain_ref,
    out_ref,
    gfull,
    ufull,
    dfull,
    xn,
    hid,
    pcs,
    pcr,
    keep,
    raws,
    rawr,
    nbs,
    nbr,
    own_acc,
    ffn,
    z_send,
    z_recv,
    y_send,
    y_recv,
    ag_send,
    ag_recv,
    pc_send,
    pc_recv,
    raw_send,
    raw_recv,
    nb_send,
    nb_recv,
):
    N_SP, N_TP = lax.axis_size("sp"), lax.axis_size("tp")
    N_X, REACH = N_TP // 2, N_SP // 2
    g = lax.axis_index("grp")
    s = lax.axis_index("sp")
    t = lax.axis_index("tp")
    core = lax.rem(t, 2)
    x = t // 2
    rows = normed_ref.shape[0]
    half = N_X * rows
    depth = gate_ref.shape[0]
    third = gate_ref.shape[1] // 3
    width = down_ref.shape[1]

    z_next = {"sp": lax.rem(s + 1, N_SP)}
    z_prev = {"sp": lax.rem(s + N_SP - 1, N_SP)}
    z_to = (z_next, z_prev)
    x_next = {"tp": lax.rem(t + 2, N_TP)}
    x_prev = {"tp": lax.rem(t + N_TP - 2, N_TP)}
    partner = {"tp": t + 1 - 2 * core}
    odd = lax.rem(g, 2)
    y_pair = {"grp": g + 1 - 2 * odd}
    mine, theirs = 2 * odd, 2 - 2 * odd

    barrier = pltpu.get_barrier_semaphore()
    for device in (z_next, z_prev, x_next, x_prev, partner, y_pair):
        pl.semaphore_signal(barrier, inc=1, device_id=device, device_id_type=MESH)
    pl.semaphore_wait(barrier, 6)

    pending = []

    def send(src, dst, ssem, rsem, device):
        copy = pltpu.make_async_remote_copy(
            src_ref=src, dst_ref=dst, send_sem=ssem, recv_sem=rsem, device_id=device, device_id_type=MESH
        )
        copy.start()
        pending.append(copy)

    def landed(dst, ssem, rsem, device):
        pltpu.make_async_remote_copy(
            src_ref=dst, dst_ref=dst, send_sem=ssem, recv_sem=rsem, device_id=device, device_id_type=MESH
        ).wait_recv()

    fulls = (gfull, ufull)
    owns = (gate_ref, up_ref)

    def place(p, j, way, part, h):
        if p < 2:
            origin = lax.rem(s + N_SP - j, N_SP) if way == 0 else lax.rem(s + j, N_SP)
            size = depth // HALVES
            at = pl.multiple_of(origin * depth + h * size, size)
            return fulls[p].at[part, pl.ds(at, size), :]
        slot, side = (0, 1) if j == REACH else (j, way)
        size = third // HALVES
        at = pl.multiple_of(part * third + h * size, size)
        return dfull.at[slot, side, pl.ds(at, size), :]

    def dest(p, j, way, part, h):
        if p < 2:
            return place(p, j, way, part, h)
        return place(p, j + 1, way, part, h)

    def own_piece(p, part, h):
        if p < 2:
            size = depth // HALVES
            return owns[p].at[pl.ds(h * size, size), pl.ds(pl.multiple_of(part * third, third), third)]
        size = third // HALVES
        return down_ref.at[pl.ds(pl.multiple_of(part * third + h * size, size), size), :]

    def zi(p, j, way, kind, h):
        return (((p * REACH + j) * 2 + way) * 2 + kind) * HALVES + h

    def yi(p, j, way, h):
        return ((p * REACH + j - 1) * 2 + way) * HALVES + h

    def travels(j, way, kind):
        return j < REACH - 1 or (j == REACH - 1 and way == kind)

    def parts(kind):
        return mine if kind == 0 else 1

    def start_own(p):
        for kind in range(2):
            for h in range(HALVES):
                for way in range(2):
                    i = zi(p, 0, way, kind, h)
                    send(
                        own_piece(p, parts(kind), h),
                        dest(p, 0, way, parts(kind), h),
                        z_send.at[i],
                        z_recv.at[i],
                        z_to[way],
                    )

    def step(pieces, j):
        for kind in range(2):
            for p in pieces:
                for h in range(HALVES):
                    for way in range(2):
                        if not travels(j - 1, way, kind):
                            continue
                        here = place(p, j, way, parts(kind), h)
                        i = zi(p, j - 1, way, kind, h)
                        landed(here, z_send.at[i], z_recv.at[i], z_to[1 - way])
                        if j < REACH and travels(j, way, kind):
                            k = zi(p, j, way, kind, h)
                            send(here, dest(p, j, way, parts(kind), h), z_send.at[k], z_recv.at[k], z_to[way])
                        if kind == 0:
                            k = yi(p, j, way, h)
                            send(here, here, y_send.at[k], y_recv.at[k], y_pair)

    def swapped(p, j):
        for way in range(2):
            if not travels(j - 1, way, 0):
                continue
            for h in range(HALVES):
                k = yi(p, j, way, h)
                landed(place(p, j, way, theirs, h), y_send.at[k], y_recv.at[k], y_pair)

    def block_of(c, xx):
        return pl.multiple_of((c * N_X + lax.rem(xx + N_X, N_X)) * rows, rows)

    start_own(0)
    start_own(1)

    h_rows = rows // 2
    ag_i = [0]

    def ag(src, dst, device):
        i = ag_i[0]
        ag_i[0] += 1
        send(src, dst, ag_send.at[i], ag_recv.at[i], device)

    def ag_wait(dst, i):
        landed(dst, ag_send.at[i], ag_recv.at[i], partner)

    own_rows = xn.at[pl.ds(block_of(core, x), rows), :]
    ag(normed_ref, own_rows, x_next)
    ag(normed_ref, own_rows, x_prev)
    ag(normed_ref, own_rows, partner)
    own_rows[...] = normed_ref[...]
    for p in range(2):
        at = pl.multiple_of(s * depth, depth)
        for k in range(3):
            fulls[p][k, pl.ds(at, depth), :] = owns[p][:, k * third : (k + 1) * third]
    dfull[0, 0] = down_ref[...]

    step((0, 1), 1)
    from_prev = xn.at[pl.ds(block_of(core, x - 1), rows), :]
    from_next = xn.at[pl.ds(block_of(core, x + 1), rows), :]
    far_low = xn.at[pl.ds(block_of(core, x + 2), h_rows), :]
    far_high = xn.at[pl.ds(pl.multiple_of(block_of(core, x + 2) + h_rows, h_rows), h_rows), :]
    ag_wait(from_prev, 0)
    low = xn.at[pl.ds(block_of(core, x - 1), h_rows), :]
    ag(low, low, x_next)
    ag(from_prev, from_prev, partner)
    ag_wait(from_next, 1)
    high = xn.at[pl.ds(pl.multiple_of(block_of(core, x + 1) + h_rows, h_rows), h_rows), :]
    ag(high, high, x_prev)
    ag(from_next, from_next, partner)
    step((0, 1), 2)
    ag_wait(far_low, 3)
    ag(far_low, far_low, partner)
    ag_wait(far_high, 5)
    ag(far_high, far_high, partner)
    step((0, 1), 3)
    other = 1 - core
    ag_wait(xn.at[pl.ds(block_of(other, x), rows), :], 2)
    ag_wait(xn.at[pl.ds(block_of(other, x - 1), rows), :], 4)
    ag_wait(xn.at[pl.ds(block_of(other, x + 1), rows), :], 6)
    ag_wait(xn.at[pl.ds(block_of(other, x + 2), h_rows), :], 7)
    ag_wait(xn.at[pl.ds(pl.multiple_of(block_of(other, x + 2) + h_rows, h_rows), h_rows), :], 8)

    for j in range(4, REACH + 1):
        step((0, 1), j)
        if j == 6:
            start_own(2)
    for p in range(2):
        for j in range(1, REACH + 1):
            swapped(p, j)

    done_down = 0
    for k in range(3):
        for b in range(2):
            piece = xn[b * half : (b + 1) * half, :]
            gate = jnp.dot(piece, gfull[k], preferred_element_type=f32)
            up = jnp.dot(piece, ufull[k], preferred_element_type=f32)
            hid[k, b * half : (b + 1) * half, :] = (gate / (1.0 + jnp.exp(-gate)) * up).astype(bf16)
            done_down += 1
            step((2,), done_down)

    order = [*range(1, REACH), 0]
    ways = ((x_next, x_prev), (x_prev, x_next))

    def product(slot, at):
        total = None
        for k in range(3):
            right = jnp.concatenate(
                [dfull[slot, side, k * third : (k + 1) * third, :] for side in range(2)], axis=1
            )
            term = jnp.dot(hid[k, pl.ds(at, half), :], right, preferred_element_type=f32)
            total = term if total is None else total + term
        return total

    def make(i):
        slot = order[i]
        if done_down_box[0] < i + 1:
            done_down_box[0] += 1
            step((2,), done_down_box[0])
        swapped(2, i + 1)
        pcs[i] = product(slot, pl.multiple_of(other * half, half)).astype(bf16)
        send(pcs.at[i], pcr.at[i], pc_send.at[i], pc_recv.at[i], partner)
        keep[i] = product(slot, pl.multiple_of(core * half, half))

    def chip_rows(i, xx, side):
        at = pl.multiple_of(lax.rem(xx + N_X, N_X) * rows, rows)
        lanes = slice(side * width, (side + 1) * width)
        return keep[i, pl.ds(at, rows), lanes] + pcr[i, pl.ds(at, rows), lanes].astype(f32)

    def spread(i):
        landed(pcr.at[i], pc_send.at[i], pc_recv.at[i], partner)
        for side in range(2):
            forth, back = ways[side]
            sign = 1 - 2 * side
            n = 2 * i + side
            raws[n] = chip_rows(i, x + 2, side).astype(bf16)
            send(raws.at[n], rawr.at[n], raw_send.at[n], raw_recv.at[n], forth)
            nbs[n, 1] = chip_rows(i, x - sign, side).astype(bf16)
            send(nbs.at[n, 1], nbr.at[n, 1], nb_send.at[2 * n + 1], nb_recv.at[2 * n + 1], back)

    def pass_on(i):
        for side in range(2):
            forth, back = ways[side]
            sign = 1 - 2 * side
            n = 2 * i + side
            landed(rawr.at[n], raw_send.at[n], raw_recv.at[n], back)
            nbs[n, 0] = (chip_rows(i, x + sign, side) + rawr[n].astype(f32)).astype(bf16)
            send(nbs.at[n, 0], nbr.at[n, 0], nb_send.at[2 * n], nb_recv.at[2 * n], forth)

    def collect(i):
        slot = order[i]
        for side in range(2):
            forth, back = ways[side]
            n = 2 * i + side
            landed(nbr.at[n, 0], nb_send.at[2 * n], nb_recv.at[2 * n], back)
            landed(nbr.at[n, 1], nb_send.at[2 * n + 1], nb_recv.at[2 * n + 1], forth)
            total = chip_rows(i, x, side) + nbr[n, 0].astype(f32) + nbr[n, 1].astype(f32)
            if slot == 0:
                origin = s if side == 0 else lax.rem(s + REACH, N_SP)
            else:
                origin = lax.rem(s + N_SP - slot, N_SP) if side == 0 else lax.rem(s + slot, N_SP)
            ffn[origin] = total

    done_down_box = [done_down]
    for i in range(REACH + 3):
        if i < REACH:
            make(i)
        if 0 <= i - 1 < REACH:
            spread(i - 1)
        if 0 <= i - 2 < REACH:
            pass_on(i - 2)
        if 0 <= i - 3 < REACH:
            collect(i - 3)

    squares = None
    for n in range(N_SP):
        v = ffn[n].astype(bf16).astype(f32)
        part = jnp.sum(v * v, axis=-1, keepdims=True)
        squares = part if squares is None else squares + part
    scale = lax.rsqrt(squares / (N_SP * width) + epsilon)
    for n in range(N_SP):
        lanes = slice(n * width, (n + 1) * width)
        v = ffn[n].astype(bf16).astype(f32)
        out_ref[:, lanes] = (
            after_ref[:, lanes].astype(f32) + 0.5 * (v * scale * gain_ref[:, lanes])
        ).astype(bf16)

    for copy in pending:
        copy.wait_send()


def feed_forward(normed, after, gate_weight, up_weight, down_weight, gain_after):
    N_SP, N_TP = lax.axis_size("sp"), lax.axis_size("tp")
    N_X, REACH = N_TP // 2, N_SP // 2
    rows, dim = normed.shape
    depth, hidden = gate_weight.shape
    width = down_weight.shape[1]
    third = hidden // 3
    half = N_X * rows
    total = N_TP * rows
    vmem = pl.BlockSpec(memory_space=pltpu.VMEM)
    dma = pltpu.SemaphoreType.DMA
    n_z = 3 * REACH * 2 * 2 * HALVES
    n_y = 3 * REACH * 2 * HALVES
    return pl.pallas_call(
        kernel,
        out_shape=jax.ShapeDtypeStruct((rows, dim), bf16),
        in_specs=[vmem] * 6,
        out_specs=vmem,
        scratch_shapes=[
            pltpu.VMEM((3, N_SP * depth, third), bf16),
            pltpu.VMEM((3, N_SP * depth, third), bf16),
            pltpu.VMEM((REACH, 2, hidden, width), bf16),
            pltpu.VMEM((total, dim), bf16),
            pltpu.VMEM((3, total, third), bf16),
            pltpu.VMEM((REACH, half, 2 * width), bf16),
            pltpu.VMEM((REACH, half, 2 * width), bf16),
            pltpu.VMEM((REACH, half, 2 * width), f32),
            pltpu.VMEM((2 * REACH, rows, width), bf16),
            pltpu.VMEM((2 * REACH, rows, width), bf16),
            pltpu.VMEM((2 * REACH, 2, rows, width), bf16),
            pltpu.VMEM((2 * REACH, 2, rows, width), bf16),
            pltpu.VMEM((8, 128), f32),
            pltpu.VMEM((N_SP, rows, width), f32),
            dma((n_z,)),
            dma((n_z,)),
            dma((n_y,)),
            dma((n_y,)),
            dma((9,)),
            dma((9,)),
            dma((REACH,)),
            dma((REACH,)),
            dma((2 * REACH,)),
            dma((2 * REACH,)),
            dma((4 * REACH,)),
            dma((4 * REACH,)),
        ],
        compiler_params=pltpu.CompilerParams(
            collective_id=0, has_side_effects=True, vmem_limit_bytes=60 * 1024 * 1024
        ),
    )(normed, after, gate_weight, up_weight, down_weight, gain_after.reshape(1, -1))


def from_everyone(shard, axis):
    size = lax.axis_size(axis)
    return lax.all_to_all(
        jnp.broadcast_to(shard[None], (size, *shard.shape)), axis, 0, 0, tiled=True
    )


def gather_directly(shard, axis, dim):
    pieces = jnp.moveaxis(from_everyone(shard, axis), 0, dim)
    lengths = pieces.shape
    return pieces.reshape(*lengths[:dim], lengths[dim] * lengths[dim + 1], *lengths[dim + 2 :])


def per_device(
    queries,
    key_rows,
    value_rows,
    doc_ids,
    sink_logits,
    out_weight,
    residual,
    gain_mixed,
    gain_before,
    gain_after,
    gate_weight,
    up_weight,
    down_weight,
):
    mixed = attend(queries, key_rows, value_rows, doc_ids, sink_logits)
    head_columns = gather_directly(out_weight, "sp", 1)
    by_rows = lax.all_to_all(mixed, "tp", split_axis=0, concat_axis=1, tiled=True)
    projected = jnp.dot(
        by_rows,
        lax.all_gather(head_columns, "tp", axis=0, tiled=True),
        preferred_element_type=jnp.float32,
    )
    projected = stored(projected)
    after = stored(residual.astype(jnp.float32) + rms_scaled(projected, gain_mixed))
    normed = rms_scaled(after, gain_before).astype(jnp.bfloat16)
    return feed_forward(
        normed, after.astype(jnp.bfloat16), gate_weight, up_weight, down_weight, gain_after
    )


def solution(mesh):
    return jax.shard_map(
        per_device,
        mesh=mesh,
        in_specs=(
            P(("grp", "sp"), "tp"),
            P(("grp", "sp"), "tp"),
            P(("grp", "sp"), "tp"),
            P(("grp", "sp")),
            P("tp"),
            P("tp", "sp"),
            P(("grp", "sp", "tp"), None),
            P(),
            P(),
            P(),
            P("sp", "tp"),
            P("sp", "tp"),
            P("tp", "sp"),
        ),
        out_specs=P(("grp", "sp", "tp"), None),
        check_vma=False,
    )
```

```python
import jax
import jax.numpy as jnp
from jax import lax
from jax.experimental import pallas as pl
from jax.experimental.pallas import tpu as pltpu
from jax.sharding import PartitionSpec as P

HEAD_DIM = 64
WINDOW = 128
epsilon = 1e-06
masked_value = -1e30
MESH = pl.DeviceIdType.MESH
f32 = jnp.float32
bf16 = jnp.bfloat16

PARTS = {"gate": 2, "up": 2, "down": 2, "out": 1}
LAGS = {"out": 0, "gate": 0, "up": 4, "down": 8}


def kernel(
    query_ref,
    key_ref,
    value_ref,
    doc_ref,
    sink_ref,
    residual_ref,
    gain_mixed_ref,
    gain_before_ref,
    gain_after_ref,
    out_weight_ref,
    gate_ref,
    up_ref,
    down_ref,
    out_ref,
    keys,
    values,
    docs,
    mixed,
    heads,
    ofull,
    gfull,
    ufull,
    dfull,
    proj,
    after,
    normed,
    xn,
    hid,
    keep,
    pcs,
    pcr,
    raws,
    rawr,
    nbs,
    nbr,
    ffn,
    halo_send,
    halo_recv,
    z_send,
    z_recv,
    y_send,
    y_recv,
    ag_send,
    ag_recv,
    pc_send,
    pc_recv,
    raw_send,
    raw_recv,
    nb_send,
    nb_recv,
):
    n_sp, n_tp = lax.axis_size("sp"), lax.axis_size("tp")
    n_x, reach = n_tp // 2, n_sp // 2
    g = lax.axis_index("grp")
    s = lax.axis_index("sp")
    t = lax.axis_index("tp")
    core = lax.rem(t, 2)
    other = 1 - core
    x = t // 2
    length = query_ref.shape[0]
    rows, dim = residual_ref.shape
    half = n_x * rows
    depth = gate_ref.shape[0]
    third = gate_ref.shape[1] // 3
    width = down_ref.shape[1]

    z_next = {"sp": lax.rem(s + 1, n_sp)}
    z_prev = {"sp": lax.rem(s + n_sp - 1, n_sp)}
    z_to = (z_next, z_prev)
    x_next = {"tp": lax.rem(t + 2, n_tp)}
    x_prev = {"tp": lax.rem(t + n_tp - 2, n_tp)}
    partner = {"tp": t + 1 - 2 * core}
    odd = lax.rem(g, 2)
    y_pair = {"grp": g + 1 - 2 * odd}
    mine, theirs = 2 * odd, 2 - 2 * odd

    barrier = pltpu.get_barrier_semaphore()
    for device in (z_next, z_prev, x_next, x_prev, partner, y_pair):
        pl.semaphore_signal(barrier, inc=1, device_id=device, device_id_type=MESH)
    pl.semaphore_wait(barrier, 6)

    pending = []

    def send(src, dst, ssem, rsem, device):
        copy = pltpu.make_async_remote_copy(
            src_ref=src, dst_ref=dst, send_sem=ssem, recv_sem=rsem, device_id=device, device_id_type=MESH
        )
        copy.start()
        pending.append(copy)

    def landed(dst, ssem, rsem, device):
        pltpu.make_async_remote_copy(
            src_ref=dst, dst_ref=dst, send_sem=ssem, recv_sem=rsem, device_id=device, device_id_type=MESH
        ).wait_recv()

    fulls = {"gate": gfull, "up": ufull}
    owns = {"gate": gate_ref, "up": up_ref}
    names = ("gate", "up", "down", "out")
    z_base, y_base, z_at, y_at = {}, {}, 0, 0
    for name in names:
        z_base[name], y_base[name] = z_at, y_at
        z_at += reach * 4 * PARTS[name]
        y_at += reach * 2 * PARTS[name]

    def place(name, j, way, part, h):
        if name in fulls:
            origin = lax.rem(s + n_sp - j, n_sp) if way == 0 else lax.rem(s + j, n_sp)
            size = depth // PARTS[name]
            at = pl.multiple_of(origin * depth + h * size, size)
            return fulls[name].at[part, pl.ds(at, size), :]
        slot, side = (0, 1) if j == reach else (j, way)
        if name == "out":
            size = out_weight_ref.shape[0] // 2
            return ofull.at[slot, side, pl.ds(part * size, size), :]
        size = third // PARTS[name]
        at = pl.multiple_of(part * third + h * size, size)
        return dfull.at[slot, side, pl.ds(at, size), :]

    def dest(name, j, way, part, h):
        return place(name, j if name in fulls else j + 1, way, part, h)

    def own_piece(name, part, h):
        if name in fulls:
            size = depth // PARTS[name]
            lanes = pl.ds(pl.multiple_of(part * third, third), third)
            return owns[name].at[pl.ds(h * size, size), lanes]
        if name == "out":
            size = out_weight_ref.shape[0] // 2
            return out_weight_ref.at[pl.ds(part * size, size), :]
        size = third // PARTS[name]
        return down_ref.at[pl.ds(pl.multiple_of(part * third + h * size, size), size), :]

    def z_sem(name, j, way, kind, h):
        return z_base[name] + ((j * 2 + way) * 2 + kind) * PARTS[name] + h

    def y_sem(name, j, way, h):
        return y_base[name] + ((j - 1) * 2 + way) * PARTS[name] + h

    def travels(j, way, kind):
        return j < reach - 1 or (j == reach - 1 and way == kind)

    def part_of(name, kind):
        if name == "out":
            return kind
        return mine if kind == 0 else 1

    def start_own(name):
        for kind in range(2):
            for h in range(PARTS[name]):
                for way in range(2):
                    i = z_sem(name, 0, way, kind, h)
                    part = part_of(name, kind)
                    send(
                        own_piece(name, part, h),
                        dest(name, 0, way, part, h),
                        z_send.at[i],
                        z_recv.at[i],
                        z_to[way],
                    )

    def step(name, j):
        for kind in range(2):
            part = part_of(name, kind)
            for h in range(PARTS[name]):
                for way in range(2):
                    if not travels(j - 1, way, kind):
                        continue
                    here = place(name, j, way, part, h)
                    i = z_sem(name, j - 1, way, kind, h)
                    landed(here, z_send.at[i], z_recv.at[i], z_to[1 - way])
                    if j < reach and travels(j, way, kind):
                        k = z_sem(name, j, way, kind, h)
                        there = dest(name, j, way, part, h)
                        send(here, there, z_send.at[k], z_recv.at[k], z_to[way])
                    if kind == 0 and name != "out":
                        k = y_sem(name, j, way, h)
                        send(here, here, y_send.at[k], y_recv.at[k], y_pair)

    def turn(r):
        for name in ("out", "gate", "up", "down"):
            if 1 <= r - LAGS[name] <= reach:
                step(name, r - LAGS[name])
        for name in ("gate", "up", "down"):
            if LAGS[name] == r:
                start_own(name)

    def swapped(name, j):
        for way in range(2):
            if not travels(j - 1, way, 0):
                continue
            for h in range(PARTS[name]):
                k = y_sem(name, j, way, h)
                landed(place(name, j, way, theirs, h), y_send.at[k], y_recv.at[k], y_pair)

    order = [*range(1, reach), 0]
    ways = ((x_next, x_prev), (x_prev, x_next))

    def origin_of(slot, side):
        if slot == 0:
            return s if side == 0 else lax.rem(s + reach, n_sp)
        return lax.rem(s + n_sp - slot, n_sp) if side == 0 else lax.rem(s + slot, n_sp)

    def summing(which, product, result):
        def slot_of(i):
            return which * reach + i

        def make(i):
            m = slot_of(i)
            pcs[m] = product(order[i], pl.multiple_of(other * half, half)).astype(bf16)
            send(pcs.at[m], pcr.at[m], pc_send.at[m], pc_recv.at[m], partner)
            keep[i] = product(order[i], pl.multiple_of(core * half, half))

        def chip_rows(i, xx, side):
            at = pl.multiple_of(lax.rem(xx + n_x, n_x) * rows, rows)
            lanes = slice(side * width, (side + 1) * width)
            return keep[i, pl.ds(at, rows), lanes] + pcr[slot_of(i), pl.ds(at, rows), lanes].astype(f32)

        def spread(i):
            m = slot_of(i)
            landed(pcr.at[m], pc_send.at[m], pc_recv.at[m], partner)
            for side in range(2):
                forth, back = ways[side]
                sign = 1 - 2 * side
                n = 2 * m + side
                raws[n] = chip_rows(i, x + 2, side).astype(bf16)
                send(raws.at[n], rawr.at[n], raw_send.at[n], raw_recv.at[n], forth)
                nbs[n, 1] = chip_rows(i, x - sign, side).astype(bf16)
                send(nbs.at[n, 1], nbr.at[n, 1], nb_send.at[2 * n + 1], nb_recv.at[2 * n + 1], back)

        def pass_on(i):
            for side in range(2):
                forth, back = ways[side]
                sign = 1 - 2 * side
                n = 2 * slot_of(i) + side
                landed(rawr.at[n], raw_send.at[n], raw_recv.at[n], back)
                nbs[n, 0] = (chip_rows(i, x + sign, side) + rawr[n].astype(f32)).astype(bf16)
                send(nbs.at[n, 0], nbr.at[n, 0], nb_send.at[2 * n], nb_recv.at[2 * n], forth)

        def collect(i):
            for side in range(2):
                forth, back = ways[side]
                n = 2 * slot_of(i) + side
                landed(nbr.at[n, 0], nb_send.at[2 * n], nb_recv.at[2 * n], back)
                landed(nbr.at[n, 1], nb_send.at[2 * n + 1], nb_recv.at[2 * n + 1], forth)
                total = chip_rows(i, x, side) + nbr[n, 0].astype(f32) + nbr[n, 1].astype(f32)
                result[origin_of(order[i], side)] = total

        return make, spread, pass_on, collect

    def block_of(c, xx):
        return pl.multiple_of((c * n_x + lax.rem(xx + n_x, n_x)) * rows, rows)

    for i, (src, dst) in enumerate(((key_ref, keys), (value_ref, values))):
        send(
            src.at[pl.ds(length - WINDOW, WINDOW), :],
            dst.at[pl.ds(0, WINDOW), :],
            halo_send.at[i],
            halo_recv.at[i],
            z_next,
        )
    send(
        doc_ref.at[:, pl.ds(length - WINDOW, WINDOW)],
        docs.at[:, pl.ds(0, WINDOW)],
        halo_send.at[2],
        halo_recv.at[2],
        z_next,
    )
    for name in ("out", "gate", "up", "down"):
        if LAGS[name] == 0:
            start_own(name)
    keys[WINDOW:, :] = key_ref[...]
    values[WINDOW:, :] = value_ref[...]
    docs[:, WINDOW:] = doc_ref[...]

    def column(row):
        return jnp.transpose(jnp.broadcast_to(row, (WINDOW, WINDOW)))

    def attend(b):
        first = b * WINDOW
        query = query_ref[first : first + WINDOW, :]
        query = jnp.concatenate([query[:, :HEAD_DIM], query[:, HEAD_DIM:]], axis=0)
        window = slice(first, first + 2 * WINDOW)
        scores = lax.dot_general(
            query, keys[window, :], (((1,), (1,)), ((), ())), preferred_element_type=f32
        ) * HEAD_DIM ** (-0.5)
        at_row = lax.broadcasted_iota(jnp.int32, (WINDOW, 2 * WINDOW), 0)
        at_col = lax.broadcasted_iota(jnp.int32, (WINDOW, 2 * WINDOW), 1)
        distance = at_row - at_col + WINDOW
        place_of_key = s * length + (first - WINDOW) + at_col
        mine_doc = column(docs[:, first + WINDOW : first + 2 * WINDOW])
        mine_doc = jnp.concatenate([mine_doc, mine_doc], axis=1)
        valid = (distance >= 0) & (distance < WINDOW) & (place_of_key >= 0)
        valid = valid & (mine_doc == docs[:, window])
        bias = jnp.where(valid, 0.0, masked_value)
        bias = jnp.concatenate([bias, bias], axis=0)
        scores = jnp.where(bias < 0.0, masked_value, scores)
        head = lax.broadcasted_iota(jnp.int32, (2 * WINDOW, 1), 0)
        sinks = jnp.where(head < WINDOW, sink_ref[0], sink_ref[1])
        top = jnp.maximum(jnp.max(scores, axis=-1, keepdims=True), sinks)
        weight = jnp.exp(scores - top)
        denom = jnp.sum(weight, axis=-1, keepdims=True) + jnp.exp(sinks - top)
        summed = jnp.dot(weight.astype(bf16), values[window, :], preferred_element_type=f32) / denom
        mixed[first : first + WINDOW, :] = jnp.concatenate(
            [summed[:WINDOW], summed[WINDOW:]], axis=1
        ).astype(bf16)

    blocks = length // WINDOW
    for b in range(1, blocks):
        attend(b)
    landed(keys.at[pl.ds(0, WINDOW), :], halo_send.at[0], halo_recv.at[0], z_prev)
    landed(values.at[pl.ds(0, WINDOW), :], halo_send.at[1], halo_recv.at[1], z_prev)
    landed(docs.at[:, pl.ds(0, WINDOW)], halo_send.at[2], halo_recv.at[2], z_prev)
    attend(0)
    for d in range(n_tp):
        u = (d % 2) * n_x + d // 2
        heads[u * rows : (u + 1) * rows, :] = mixed[d * rows : (d + 1) * rows, :]
    ofull[0, 0] = out_weight_ref[...]

    def project(slot, at):
        right = jnp.concatenate([ofull[slot, side] for side in range(2)], axis=1)
        return jnp.dot(heads[pl.ds(at, half), :], right, preferred_element_type=f32)

    make, spread, pass_on, collect = summing(0, project, proj)
    for i in range(reach + 3):
        turn(i + 1)
        if i < reach:
            make(i)
        if 0 <= i - 1 < reach:
            spread(i - 1)
        if 0 <= i - 2 < reach:
            pass_on(i - 2)
        if 0 <= i - 3 < reach:
            collect(i - 3)

    for name in fulls:
        at = pl.multiple_of(s * depth, depth)
        for k in range(3):
            fulls[name][k, pl.ds(at, depth), :] = owns[name][:, k * third : (k + 1) * third]
    dfull[0, 0] = down_ref[...]

    def scale_of(squares):
        return lax.rsqrt(squares / dim + epsilon)

    squares = None
    for n in range(n_sp):
        v = proj[n].astype(bf16).astype(f32)
        part = jnp.sum(v * v, axis=-1, keepdims=True)
        squares = part if squares is None else squares + part
    scale = scale_of(squares)
    squares = None
    for n in range(n_sp):
        lanes = slice(n * width, (n + 1) * width)
        v = proj[n].astype(bf16).astype(f32)
        v = residual_ref[:, lanes].astype(f32) + v * scale * gain_mixed_ref[:, lanes]
        v = v.astype(bf16)
        after[:, lanes] = v
        v = v.astype(f32)
        part = jnp.sum(v * v, axis=-1, keepdims=True)
        squares = part if squares is None else squares + part
    scale = scale_of(squares)
    for n in range(n_sp):
        lanes = slice(n * width, (n + 1) * width)
        v = after[:, lanes].astype(f32)
        normed[:, lanes] = (v * scale * gain_before_ref[:, lanes]).astype(bf16)

    h_rows = rows // 2
    ag_at = {}

    def row_part(c, xx, h):
        return xn.at[pl.ds(pl.multiple_of(block_of(c, xx) + h * h_rows, h_rows), h_rows), :]

    def ag_send_to(key, src, dst, device):
        i = ag_at[key] = len(ag_at)
        send(src, dst, ag_send.at[i], ag_recv.at[i], device)

    def ag_wait(key, dst):
        landed(dst, ag_send.at[ag_at[key]], ag_recv.at[ag_at[key]], partner)

    for h in range(2):
        src = normed.at[pl.ds(h * h_rows, h_rows), :]
        ag_send_to(("next", h), src, row_part(core, x, h), x_next)
        src = normed.at[pl.ds((1 - h) * h_rows, h_rows), :]
        ag_send_to(("prev", 1 - h), src, row_part(core, x, 1 - h), x_prev)
        src = normed.at[pl.ds(h * h_rows, h_rows), :]
        ag_send_to(("own", h), src, row_part(core, x, h), partner)
    xn[pl.ds(block_of(core, x), rows), :] = normed[...]

    def relay(h):
        for key, hh, xx, far, to in (("next", h, x - 1, 0, x_next), ("prev", 1 - h, x + 1, 1, x_prev)):
            here = row_part(core, xx, hh)
            ag_wait((key, hh), here)
            if hh == far:
                ag_send_to(("far", hh), here, here, to)
            ag_send_to((key, hh, "partner"), here, here, partner)

    def relay_far(h):
        here = row_part(core, x + 2, h)
        ag_wait(("far", h), here)
        ag_send_to(("far", h, "partner"), here, here, partner)

    last = reach + 3
    turn(last + 1)
    relay(0)
    turn(last + 2)
    relay(1)
    turn(last + 3)
    relay_far(0)
    relay_far(1)
    for h in range(2):
        ag_wait(("own", h), row_part(other, x, h))
        ag_wait(("next", h, "partner"), row_part(other, x - 1, h))
        ag_wait(("prev", h, "partner"), row_part(other, x + 1, h))
        ag_wait(("far", h, "partner"), row_part(other, x + 2, h))

    last = max(last + 3, LAGS["gate"] + reach, LAGS["up"] + reach)
    for r in range(reach + 7, last + 1):
        turn(r)
    for j in range(1, reach + 1):
        swapped("gate", j)
    for j in range(1, reach + 1):
        swapped("up", j)

    for k in range(3):
        for b in range(2):
            piece = xn[b * half : (b + 1) * half, :]
            gate = jnp.dot(piece, gfull[k], preferred_element_type=f32)
            up = jnp.dot(piece, ufull[k], preferred_element_type=f32)
            hid[k, b * half : (b + 1) * half, :] = (gate / (1.0 + jnp.exp(-gate)) * up).astype(bf16)
            last += 1
            turn(last)

    def lower(slot, at):
        total = None
        for k in range(3):
            right = jnp.concatenate(
                [dfull[slot, side, k * third : (k + 1) * third, :] for side in range(2)], axis=1
            )
            term = jnp.dot(hid[k, pl.ds(at, half), :], right, preferred_element_type=f32)
            total = term if total is None else total + term
        return total

    make, spread, pass_on, collect = summing(1, lower, ffn)
    for i in range(reach + 3):
        while last < i + 1 + LAGS["down"] and i < reach:
            last += 1
            turn(last)
        if i < reach:
            swapped("down", i + 1)
            make(i)
        if 0 <= i - 1 < reach:
            spread(i - 1)
        if 0 <= i - 2 < reach:
            pass_on(i - 2)
        if 0 <= i - 3 < reach:
            collect(i - 3)

    squares = None
    for n in range(n_sp):
        v = ffn[n].astype(bf16).astype(f32)
        part = jnp.sum(v * v, axis=-1, keepdims=True)
        squares = part if squares is None else squares + part
    scale = scale_of(squares)
    for n in range(n_sp):
        lanes = slice(n * width, (n + 1) * width)
        v = ffn[n].astype(bf16).astype(f32)
        out_ref[:, lanes] = (
            after[:, lanes].astype(f32) + 0.5 * (v * scale * gain_after_ref[:, lanes])
        ).astype(bf16)

    for copy in pending:
        copy.wait_send()


def per_device(
    queries,
    key_rows,
    value_rows,
    doc_ids,
    sink_logits,
    out_weight,
    residual,
    gain_mixed,
    gain_before,
    gain_after,
    gate_weight,
    up_weight,
    down_weight,
):
    n_sp, n_tp = lax.axis_size("sp"), lax.axis_size("tp")
    n_x, reach = n_tp // 2, n_sp // 2
    length = queries.shape[0]
    rows, dim = residual.shape
    depth, hidden = gate_weight.shape
    width = down_weight.shape[1]
    third = hidden // 3
    half = n_x * rows
    vmem = pl.BlockSpec(memory_space=pltpu.VMEM)
    smem = pl.BlockSpec(memory_space=pltpu.SMEM)
    dma = pltpu.SemaphoreType.DMA
    pieces = sum(PARTS.values())
    return pl.pallas_call(
        kernel,
        out_shape=jax.ShapeDtypeStruct((rows, dim), bf16),
        in_specs=[vmem] * 4 + [smem] + [vmem] * 8,
        out_specs=vmem,
        scratch_shapes=[
            pltpu.VMEM((length + WINDOW, key_rows.shape[1]), bf16),
            pltpu.VMEM((length + WINDOW, value_rows.shape[1]), bf16),
            pltpu.VMEM((1, length + WINDOW), jnp.int32),
            pltpu.VMEM(queries.shape, bf16),
            pltpu.VMEM(queries.shape, bf16),
            pltpu.VMEM((reach, 2, *out_weight.shape), bf16),
            pltpu.VMEM((3, n_sp * depth, third), bf16),
            pltpu.VMEM((3, n_sp * depth, third), bf16),
            pltpu.VMEM((reach, 2, hidden, width), bf16),
            pltpu.VMEM((n_sp, rows, width), f32),
            pltpu.VMEM((rows, dim), bf16),
            pltpu.VMEM((rows, dim), bf16),
            pltpu.VMEM((length, dim), bf16),
            pltpu.VMEM((3, length, third), bf16),
            pltpu.VMEM((reach, half, 2 * width), f32),
            pltpu.VMEM((2 * reach, half, 2 * width), bf16),
            pltpu.VMEM((2 * reach, half, 2 * width), bf16),
            pltpu.VMEM((4 * reach, rows, width), bf16),
            pltpu.VMEM((4 * reach, rows, width), bf16),
            pltpu.VMEM((4 * reach, 2, rows, width), bf16),
            pltpu.VMEM((4 * reach, 2, rows, width), bf16),
            pltpu.VMEM((n_sp, rows, width), f32),
            dma((3,)),
            dma((3,)),
            dma((4 * reach * pieces,)),
            dma((4 * reach * pieces,)),
            dma((2 * reach * pieces,)),
            dma((2 * reach * pieces,)),
            dma((14,)),
            dma((14,)),
            dma((2 * reach,)),
            dma((2 * reach,)),
            dma((4 * reach,)),
            dma((4 * reach,)),
            dma((8 * reach,)),
            dma((8 * reach,)),
        ],
        compiler_params=pltpu.CompilerParams(
            collective_id=0, has_side_effects=True, vmem_limit_bytes=60 * 1024 * 1024
        ),
    )(
        queries,
        key_rows,
        value_rows,
        doc_ids.reshape(1, -1),
        sink_logits,
        residual,
        gain_mixed.reshape(1, -1),
        gain_before.reshape(1, -1),
        gain_after.reshape(1, -1),
        out_weight,
        gate_weight,
        up_weight,
        down_weight,
    )


def solution(mesh):
    return jax.shard_map(
        per_device,
        mesh=mesh,
        in_specs=(
            P(("grp", "sp"), "tp"),
            P(("grp", "sp"), "tp"),
            P(("grp", "sp"), "tp"),
            P(("grp", "sp")),
            P("tp"),
            P("tp", "sp"),
            P(("grp", "sp", "tp"), None),
            P(),
            P(),
            P(),
            P("sp", "tp"),
            P("sp", "tp"),
            P("tp", "sp"),
        ),
        out_specs=P(("grp", "sp", "tp"), None),
        check_vma=False,
    )
```

```python
import functools

import jax
import jax.numpy as jnp
from jax import lax
from jax.experimental import pallas as pl
from jax.experimental.pallas import tpu as pltpu
from jax.sharding import PartitionSpec as P

HEAD_DIM = 64
WINDOW = 128
epsilon = 1e-06
masked_value = -1e30
MESH = pl.DeviceIdType.MESH
f32 = jnp.float32
bf16 = jnp.bfloat16

PARTS = {"gate": 2, "up": 2, "down": 2, "out": 1}
STREAMS = (
    ("out", 0, 0),
    ("out", 1, 0),
    ("gate", 0, 0),
    ("gate", 1, 0),
    ("up", 0, 0),
    ("up", 1, 4),
    ("down", 0, 6),
    ("down", 1, 8),
)


def kernel(
    query_ref,
    key_ref,
    value_ref,
    doc_ref,
    sink_ref,
    residual_ref,
    gain_mixed_ref,
    gain_before_ref,
    gain_after_ref,
    out_weight_ref,
    gate_ref,
    up_ref,
    down_ref,
    out_ref,
    keys,
    values,
    docs,
    mixed,
    heads,
    ofull,
    gfull,
    ufull,
    dfull,
    proj,
    after,
    normed,
    xn,
    hid,
    keep,
    pcs,
    pcr,
    raws,
    rawr,
    nbs,
    nbr,
    ffn,
    halo_send,
    halo_recv,
    z_send,
    z_recv,
    y_send,
    y_recv,
    ag_send,
    ag_recv,
    pc_send,
    pc_recv,
    raw_send,
    raw_recv,
    nb_send,
    nb_recv,
):
    n_sp, n_tp = lax.axis_size("sp"), lax.axis_size("tp")
    n_x, reach = n_tp // 2, n_sp // 2
    g = lax.axis_index("grp")
    s = lax.axis_index("sp")
    t = lax.axis_index("tp")
    core = lax.rem(t, 2)
    other = 1 - core
    x = t // 2
    length = query_ref.shape[0]
    rows, dim = residual_ref.shape
    half = n_x * rows
    depth = gate_ref.shape[0]
    third = gate_ref.shape[1] // 3
    width = down_ref.shape[1]

    z_next = {"sp": lax.rem(s + 1, n_sp)}
    z_prev = {"sp": lax.rem(s + n_sp - 1, n_sp)}
    z_to = (z_next, z_prev)
    x_next = {"tp": lax.rem(t + 2, n_tp)}
    x_prev = {"tp": lax.rem(t + n_tp - 2, n_tp)}
    partner = {"tp": t + 1 - 2 * core}
    odd = lax.rem(g, 2)
    y_pair = {"grp": g + 1 - 2 * odd}
    mine, theirs = 2 * odd, 2 - 2 * odd

    barrier = pltpu.get_barrier_semaphore()
    for device in (z_next, z_prev, x_next, x_prev, partner, y_pair):
        pl.semaphore_signal(barrier, inc=1, device_id=device, device_id_type=MESH)
    pl.semaphore_wait(barrier, 6)

    def send(src, dst, ssem, rsem, device):
        pltpu.make_async_remote_copy(
            src_ref=src, dst_ref=dst, send_sem=ssem, recv_sem=rsem, device_id=device, device_id_type=MESH
        ).start()

    def sent(size, ssem):
        pltpu.make_async_remote_copy(
            src_ref=size, dst_ref=size, send_sem=ssem, recv_sem=ssem, device_id=partner, device_id_type=MESH
        ).wait_send()

    def landed(dst, ssem, rsem, device):
        pltpu.make_async_remote_copy(
            src_ref=dst, dst_ref=dst, send_sem=ssem, recv_sem=rsem, device_id=device, device_id_type=MESH
        ).wait_recv()

    fulls = {"gate": gfull, "up": ufull}
    owns = {"gate": gate_ref, "up": up_ref}
    names = ("gate", "up", "down", "out")
    z_base, z_at = {}, 0
    for name in names:
        z_base[name] = z_at
        z_at += reach * 2 * PARTS[name]

    def place(name, j, way, part, h):
        if name in fulls:
            origin = lax.rem(s + n_sp - j, n_sp) if way == 0 else lax.rem(s + j, n_sp)
            size = depth // PARTS[name]
            at = pl.multiple_of(origin * depth + h * size, size)
            return fulls[name].at[part, pl.ds(at, size), :]
        slot, side = (0, 1) if j == reach else (j, way)
        if name == "out":
            size = out_weight_ref.shape[0] // 2
            return ofull.at[slot, side, pl.ds(part * size, size), :]
        size = third // PARTS[name]
        at = pl.multiple_of(part * third + h * size, size)
        return dfull.at[slot, side, pl.ds(at, size), :]

    def dest(name, j, way, part, h):
        return place(name, j if name in fulls else j + 1, way, part, h)

    def own_piece(name, part, h):
        if name in fulls:
            size = depth // PARTS[name]
            lanes = pl.ds(pl.multiple_of(part * third, third), third)
            return owns[name].at[pl.ds(h * size, size), lanes]
        if name == "out":
            size = out_weight_ref.shape[0] // 2
            return out_weight_ref.at[pl.ds(part * size, size), :]
        size = third // PARTS[name]
        return down_ref.at[pl.ds(pl.multiple_of(part * third + h * size, size), size), :]

    def z_sem(name, j, kind, h):
        return z_recv.at[z_base[name] + (j * 2 + kind) * PARTS[name] + h]

    def y_sem(name, j):
        return y_recv.at[names.index(name) if name in fulls else 1 + j]

    def travels(j, way, kind):
        return j < reach - 1 or (j == reach - 1 and way == kind)

    def part_of(name, kind):
        if name == "out":
            return kind
        return mine if kind == 0 else 1

    def start_own(name, kind):
        part = part_of(name, kind)
        for h in range(PARTS[name]):
            for way in range(2):
                there = dest(name, 0, way, part, h)
                which = z_send.at[names.index(name)]
                send(own_piece(name, part, h), there, which, z_sem(name, 0, kind, h), z_to[way])

    def step(name, kind, j):
        part = part_of(name, kind)
        which = names.index(name)
        ends = [way for way in range(2) if travels(j - 1, way, kind)]
        for h in range(PARTS[name]):
            landed(as_many(name, len(ends)), z_send.at[which], z_sem(name, j - 1, kind, h), z_next)
            for way in ends:
                here = place(name, j, way, part, h)
                if j < reach and travels(j, way, kind):
                    there = dest(name, j, way, part, h)
                    send(here, there, z_send.at[which], z_sem(name, j, kind, h), z_to[way])
                if kind == 0 and name != "out":
                    send(here, here, y_send.at[which], y_sem(name, j), y_pair)

    def as_many(name, count):
        if name in fulls:
            return fulls[name].at[0, pl.ds(0, count * (depth // PARTS[name])), :]
        if name == "out":
            return ofull.at[0, 0, pl.ds(0, count * (out_weight_ref.shape[0] // 2)), :]
        return dfull.at[0, 0, pl.ds(0, count * (third // PARTS[name])), :]

    def steps_of(r):
        todo = []
        for name, kind, lag in STREAMS:
            if 1 <= r - lag <= reach:
                todo.append(functools.partial(step, name, kind, r - lag))
        for name, kind, lag in STREAMS:
            if 0 < lag == r:
                todo.append(functools.partial(start_own, name, kind))
        return todo

    rounds = max(lag for _, _, lag in STREAMS) + reach
    waiting = [(r, todo) for r in range(1, rounds + 1) for todo in steps_of(r)]

    def serve(count):
        for _ in range(min(count, len(waiting))):
            waiting.pop(0)[1]()

    def serve_through(r):
        while waiting and waiting[0][0] <= r:
            waiting.pop(0)[1]()

    def serve_until(name, j):
        while any(
            todo.func is step and todo.args[0] == name and todo.args[2] <= j for _, todo in waiting
        ):
            waiting.pop(0)[1]()

    def swapped(name, j=1):
        which = names.index(name)
        if name in fulls:
            size = fulls[name].at[0, pl.ds(0, (n_sp - 1) * depth), :]
        else:
            size = dfull.at[0, 0, pl.ds(0, (2 if j < reach else 1) * third), :]
        landed(size, y_send.at[which], y_sem(name, j), y_pair)

    order = [*range(1, reach), 0]
    ways = ((x_next, x_prev), (x_prev, x_next))

    def origin_of(slot, side):
        if slot == 0:
            return s if side == 0 else lax.rem(s + reach, n_sp)
        return lax.rem(s + n_sp - slot, n_sp) if side == 0 else lax.rem(s + slot, n_sp)

    def summing(which, product, result):
        def slot_of(i):
            return which * reach + i

        def make(i):
            m = slot_of(i)
            pcs[m] = product(order[i], pl.multiple_of(other * half, half)).astype(bf16)
            send(pcs.at[m], pcr.at[m], pc_send.at[0], pc_recv.at[i], partner)
            keep[i] = product(order[i], pl.multiple_of(core * half, half))

        def chip_rows(i, xx, side):
            at = pl.multiple_of(lax.rem(xx + n_x, n_x) * rows, rows)
            lanes = slice(side * width, (side + 1) * width)
            return keep[i, pl.ds(at, rows), lanes] + pcr[slot_of(i), pl.ds(at, rows), lanes].astype(f32)

        def spread(i):
            m = slot_of(i)
            landed(pcr.at[m], pc_send.at[0], pc_recv.at[i], partner)
            for side in range(2):
                forth, back = ways[side]
                sign = 1 - 2 * side
                raws[m, side] = chip_rows(i, x + 2, side).astype(bf16)
                send(raws.at[m, side], rawr.at[m, side], raw_send.at[0], raw_recv.at[i], forth)
                nbs[m, side, 1] = chip_rows(i, x - sign, side).astype(bf16)
                send(nbs.at[m, side, 1], nbr.at[m, side, 1], nb_send.at[0], nb_recv.at[i], back)

        def pass_on(i):
            m = slot_of(i)
            landed(rawr.at[m], raw_send.at[0], raw_recv.at[i], x_next)
            for side in range(2):
                forth, back = ways[side]
                sign = 1 - 2 * side
                nbs[m, side, 0] = (chip_rows(i, x + sign, side) + rawr[m, side].astype(f32)).astype(bf16)
                send(nbs.at[m, side, 0], nbr.at[m, side, 0], nb_send.at[0], nb_recv.at[i], forth)

        def collect(i):
            m = slot_of(i)
            landed(nbr.at[m], nb_send.at[0], nb_recv.at[i], x_next)
            for side in range(2):
                total = chip_rows(i, x, side) + nbr[m, side, 0].astype(f32)
                result[origin_of(order[i], side)] = total + nbr[m, side, 1].astype(f32)

        return make, spread, pass_on, collect

    def block_of(c, xx):
        return pl.multiple_of((c * n_x + lax.rem(xx + n_x, n_x)) * rows, rows)

    blocks = length // WINDOW
    docs[0] = doc_ref[blocks - 1 : blocks, :]
    for i, (src, dst) in enumerate(((key_ref, keys), (value_ref, values))):
        send(
            src.at[:, pl.ds(length - WINDOW, WINDOW)],
            dst.at[:, pl.ds(0, WINDOW)],
            halo_send.at[i],
            halo_recv.at[i],
            z_next,
        )
    send(docs.at[0], docs.at[1], halo_send.at[2], halo_recv.at[2], z_next)
    for name, kind, lag in STREAMS:
        if lag == 0:
            start_own(name, kind)
    keys[:, WINDOW:] = key_ref[...]
    values[:, WINDOW:] = value_ref[...]

    def column(row):
        return jnp.transpose(jnp.broadcast_to(row, (WINDOW, WINDOW)))

    def attend(b):
        first = b * WINDOW
        query = query_ref[first : first + WINDOW, :]
        query = jnp.concatenate([query[:, :HEAD_DIM], query[:, HEAD_DIM:]], axis=0)
        window = slice(first, first + 2 * WINDOW)
        scores = jnp.dot(query, keys[:, window], preferred_element_type=f32) * HEAD_DIM ** (-0.5)
        at_row = lax.broadcasted_iota(jnp.int32, (WINDOW, 2 * WINDOW), 0)
        at_col = lax.broadcasted_iota(jnp.int32, (WINDOW, 2 * WINDOW), 1)
        distance = at_row - at_col + WINDOW
        place_of_key = s * length + (first - WINDOW) + at_col
        own_doc = doc_ref[b : b + 1, :]
        mine_doc = column(own_doc)
        mine_doc = jnp.concatenate([mine_doc, mine_doc], axis=1)
        earlier = docs[1] if b == 0 else doc_ref[b - 1 : b, :]
        valid = (distance >= 0) & (distance < WINDOW) & (place_of_key >= 0)
        valid = valid & (mine_doc == jnp.concatenate([earlier, own_doc], axis=1))
        bias = jnp.where(valid, 0.0, masked_value)
        bias = jnp.concatenate([bias, bias], axis=0)
        scores = jnp.where(bias < 0.0, masked_value, scores)
        head = lax.broadcasted_iota(jnp.int32, (2 * WINDOW, 1), 0)
        sinks = jnp.where(head < WINDOW, sink_ref[0], sink_ref[1])
        top = jnp.maximum(jnp.max(scores, axis=-1, keepdims=True), sinks)
        weight = jnp.exp(scores - top)
        denom = jnp.sum(weight, axis=-1, keepdims=True) + jnp.exp(sinks - top)
        summed = lax.dot_general(
            weight.astype(bf16),
            values[:, window],
            (((1,), (1,)), ((), ())),
            preferred_element_type=f32,
        ) / denom
        mixed[first : first + WINDOW, :] = jnp.concatenate(
            [summed[:WINDOW], summed[WINDOW:]], axis=1
        ).astype(bf16)

    for b in range(1, blocks):
        attend(b)
    landed(keys.at[:, pl.ds(0, WINDOW)], halo_send.at[0], halo_recv.at[0], z_prev)
    landed(values.at[:, pl.ds(0, WINDOW)], halo_send.at[1], halo_recv.at[1], z_prev)
    landed(docs.at[1], halo_send.at[2], halo_recv.at[2], z_prev)
    attend(0)
    for d in range(n_tp):
        u = (d % 2) * n_x + d // 2
        heads[u * rows : (u + 1) * rows, :] = mixed[d * rows : (d + 1) * rows, :]
    ofull[0, 0] = out_weight_ref[...]

    def project(slot, at):
        right = jnp.concatenate([ofull[slot, side] for side in range(2)], axis=1)
        return jnp.dot(heads[pl.ds(at, half), :], right, preferred_element_type=f32)

    make, spread, pass_on, collect = summing(0, project, proj)
    for i in range(reach):
        serve_until("out", i + 1)
        make(i)
        if i >= 1:
            pass_on(i - 1)
        serve(1)
        spread(i)
        if i >= 1:
            collect(i - 1)
        serve_through(i + 1)
    serve(1)
    pass_on(reach - 1)
    serve(2)
    collect(reach - 1)

    for name in fulls:
        at = pl.multiple_of(s * depth, depth)
        for k in range(3):
            fulls[name][k, pl.ds(at, depth), :] = owns[name][:, k * third : (k + 1) * third]
    dfull[0, 0] = down_ref[...]

    def scale_of(squares):
        return lax.rsqrt(squares / dim + epsilon)

    def normalise():
        squares = None
        for n in range(n_sp):
            v = proj[n].astype(bf16).astype(f32)
            part = jnp.sum(v * v, axis=-1, keepdims=True)
            squares = part if squares is None else squares + part
        scale = scale_of(squares)
        squares = None
        for n in range(n_sp):
            lanes = slice(n * width, (n + 1) * width)
            v = proj[n].astype(bf16).astype(f32)
            v = residual_ref[:, lanes].astype(f32) + v * scale * gain_mixed_ref[:, lanes]
            v = v.astype(bf16)
            after[:, lanes] = v
            v = v.astype(f32)
            part = jnp.sum(v * v, axis=-1, keepdims=True)
            squares = part if squares is None else squares + part
        scale = scale_of(squares)
        for n in range(n_sp):
            lanes = slice(n * width, (n + 1) * width)
            v = after[:, lanes].astype(f32)
            normed[:, lanes] = (v * scale * gain_before_ref[:, lanes]).astype(bf16)

    normalise()

    h_rows = rows // 2
    ag_at = {}

    def row_part(c, xx, h):
        return xn.at[pl.ds(pl.multiple_of(block_of(c, xx) + h * h_rows, h_rows), h_rows), :]

    def ag_send_to(key, src, dst, device):
        if key not in ag_at:
            ag_at[key] = len(ag_at)
        send(src, dst, ag_send.at[0], ag_recv.at[ag_at[key]], device)

    def ag_wait(key, dst):
        landed(dst, ag_send.at[0], ag_recv.at[ag_at[key]], partner)

    for h in range(2):
        src = normed.at[pl.ds(h * h_rows, h_rows), :]
        ag_send_to(("next", h), src, row_part(core, x, h), x_next)
        src = normed.at[pl.ds((1 - h) * h_rows, h_rows), :]
        ag_send_to(("prev", 1 - h), src, row_part(core, x, 1 - h), x_prev)
        src = normed.at[pl.ds(h * h_rows, h_rows), :]
        ag_send_to("partner", src, row_part(core, x, h), partner)
    xn[pl.ds(block_of(core, x), rows), :] = normed[...]

    def relay(h):
        for key, hh, xx, far, to in (("next", h, x - 1, 0, x_next), ("prev", 1 - h, x + 1, 1, x_prev)):
            here = row_part(core, xx, hh)
            ag_wait((key, hh), here)
            if hh == far:
                ag_send_to(("far", hh), here, here, to)
            ag_send_to("partner", here, here, partner)

    def relay_far(h):
        here = row_part(core, x + 2, h)
        ag_wait(("far", h), here)
        ag_send_to("partner", here, here, partner)

    serve(4)
    relay(0)
    serve(4)
    relay(1)
    serve(4)
    relay_far(0)
    relay_far(1)
    ag_wait("partner", xn.at[pl.ds(block_of(other, 0), half), :])
    serve_until("gate", reach)
    serve_until("up", reach)
    swapped("gate")
    swapped("up")

    def units(k, b):
        piece = xn[b * half : (b + 1) * half, :]
        gate = jnp.dot(piece, gfull[k], preferred_element_type=f32)
        up = jnp.dot(piece, ufull[k], preferred_element_type=f32)
        hid[k, b * half : (b + 1) * half, :] = (gate / (1.0 + jnp.exp(-gate)) * up).astype(bf16)

    for k in range(3):
        for b in range(2):
            units(k, b)
            serve(1)

    def lower(slot, at):
        total = None
        for k in range(3):
            right = jnp.concatenate(
                [dfull[slot, side, k * third : (k + 1) * third, :] for side in range(2)], axis=1
            )
            term = jnp.dot(hid[k, pl.ds(at, half), :], right, preferred_element_type=f32)
            total = term if total is None else total + term
        return total

    make, spread, pass_on, collect = summing(1, lower, ffn)
    for i in range(reach + 7):
        if i < reach:
            serve_until("down", i + 1)
            swapped("down", i + 1)
            make(i)
        if 0 <= i - 1 < reach:
            spread(i - 1)
        if 0 <= i - 4 < reach:
            pass_on(i - 4)
        if 0 <= i - 7 < reach:
            collect(i - 7)

    def finish():
        squares = None
        for n in range(n_sp):
            v = ffn[n].astype(bf16).astype(f32)
            part = jnp.sum(v * v, axis=-1, keepdims=True)
            squares = part if squares is None else squares + part
        scale = scale_of(squares)
        for n in range(n_sp):
            lanes = slice(n * width, (n + 1) * width)
            v = ffn[n].astype(bf16).astype(f32)
            out_ref[:, lanes] = (
                after[:, lanes].astype(f32) + 0.5 * (v * scale * gain_after_ref[:, lanes])
            ).astype(bf16)

    finish()

    def drain():
        trips = n_sp - 1
        shard = gfull.at[pl.ds(0, 2), pl.ds(0, trips * depth), :]
        swap = gfull.at[0, pl.ds(0, trips * depth), :]
        for i, name in enumerate(names):
            if name == "out":
                sent(gfull.at[0, pl.ds(0, trips * depth // 2), :], z_send.at[i])
            else:
                sent(shard, z_send.at[i])
                sent(swap, y_send.at[i])
        sent(xn.at[pl.ds(0, length - rows), :], ag_send.at[0])
        sent(pcs, pc_send.at[0])
        sent(raws, raw_send.at[0])
        sent(nbs, nb_send.at[0])
        tail = pl.ds(0, WINDOW)
        sent(keys.at[:, tail], halo_send.at[0])
        sent(values.at[:, tail], halo_send.at[1])
        sent(docs.at[0], halo_send.at[2])

    drain()


def per_device(
    queries,
    key_rows,
    value_rows,
    doc_ids,
    sink_logits,
    out_weight,
    residual,
    gain_mixed,
    gain_before,
    gain_after,
    gate_weight,
    up_weight,
    down_weight,
):
    n_sp, n_tp = lax.axis_size("sp"), lax.axis_size("tp")
    n_x, reach = n_tp // 2, n_sp // 2
    length = queries.shape[0]
    rows, dim = residual.shape
    depth, hidden = gate_weight.shape
    width = down_weight.shape[1]
    third = hidden // 3
    half = n_x * rows
    vmem = pl.BlockSpec(memory_space=pltpu.VMEM)
    smem = pl.BlockSpec(memory_space=pltpu.SMEM)
    dma = pltpu.SemaphoreType.DMA
    pieces = sum(PARTS.values())
    return pl.pallas_call(
        kernel,
        out_shape=jax.ShapeDtypeStruct((rows, dim), bf16),
        in_specs=[vmem] * 4 + [smem] + [vmem] * 8,
        out_specs=vmem,
        scratch_shapes=[
            pltpu.VMEM((key_rows.shape[1], length + WINDOW), bf16),
            pltpu.VMEM((value_rows.shape[1], length + WINDOW), bf16),
            pltpu.VMEM((2, 1, WINDOW), jnp.int32),
            pltpu.VMEM(queries.shape, bf16),
            pltpu.VMEM(queries.shape, bf16),
            pltpu.VMEM((reach, 2, *out_weight.shape), bf16),
            pltpu.VMEM((3, n_sp * depth, third), bf16),
            pltpu.VMEM((3, n_sp * depth, third), bf16),
            pltpu.VMEM((reach, 2, hidden, width), bf16),
            pltpu.VMEM((n_sp, rows, width), f32),
            pltpu.VMEM((rows, dim), bf16),
            pltpu.VMEM((rows, dim), bf16),
            pltpu.VMEM((length, dim), bf16),
            pltpu.VMEM((3, length, third), bf16),
            pltpu.VMEM((reach, half, 2 * width), f32),
            pltpu.VMEM((2 * reach, half, 2 * width), bf16),
            pltpu.VMEM((2 * reach, half, 2 * width), bf16),
            pltpu.VMEM((2 * reach, 2, rows, width), bf16),
            pltpu.VMEM((2 * reach, 2, rows, width), bf16),
            pltpu.VMEM((2 * reach, 2, 2, rows, width), bf16),
            pltpu.VMEM((2 * reach, 2, 2, rows, width), bf16),
            pltpu.VMEM((n_sp, rows, width), f32),
            dma((3,)),
            dma((3,)),
            dma((4,)),
            dma((2 * reach * pieces,)),
            dma((3,)),
            dma((2 + reach,)),
            dma((1,)),
            dma((7,)),
            dma((1,)),
            dma((reach,)),
            dma((1,)),
            dma((reach,)),
            dma((1,)),
            dma((reach,)),
        ],
        compiler_params=pltpu.CompilerParams(
            collective_id=0, has_side_effects=True, vmem_limit_bytes=60 * 1024 * 1024
        ),
    )(
        queries,
        key_rows.T,
        value_rows.T,
        doc_ids.reshape(-1, WINDOW),
        sink_logits,
        residual,
        gain_mixed.reshape(1, -1),
        gain_before.reshape(1, -1),
        gain_after.reshape(1, -1),
        out_weight,
        gate_weight,
        up_weight,
        down_weight,
    )


def solution(mesh):
    return jax.shard_map(
        per_device,
        mesh=mesh,
        in_specs=(
            P(("grp", "sp"), "tp"),
            P(("grp", "sp"), "tp"),
            P(("grp", "sp"), "tp"),
            P(("grp", "sp")),
            P("tp"),
            P("tp", "sp"),
            P(("grp", "sp", "tp"), None),
            P(),
            P(),
            P(),
            P("sp", "tp"),
            P("sp", "tp"),
            P("tp", "sp"),
        ),
        out_specs=P(("grp", "sp", "tp"), None),
        check_vma=False,
    )
```

```python
import functools

import jax
import jax.numpy as jnp
from jax import lax
from jax.experimental import pallas as pl
from jax.experimental.pallas import tpu as pltpu
from jax.sharding import PartitionSpec as P

HEAD_DIM = 64
WINDOW = 128
epsilon = 1e-06
masked_value = -1e30
MESH = pl.DeviceIdType.MESH
f32 = jnp.float32
bf16 = jnp.bfloat16

PARTS = {"gate": 2, "up": 2, "down": 2, "out": 1}
STREAMS = (
    ("out", 0, 0),
    ("out", 1, 0),
    ("gate", 0, 0),
    ("gate", 1, 4),
    ("up", 0, 0),
    ("up", 1, 5),
    ("down", 0, 7),
    ("down", 1, 7),
)
SERVE_RS = (2, 2, 1)
SERVE_AG = (5, 3, 3, 2)
SERVE_UNITS = 1


def kernel(
    query_ref,
    key_ref,
    value_ref,
    doc_ref,
    sink_ref,
    residual_hbm,
    gain_mixed_ref,
    gain_before_ref,
    gain_after_ref,
    out_weight_ref,
    gate_ref,
    up_ref,
    down_ref,
    out_ref,
    keys,
    values,
    docs,
    mixed,
    heads,
    ofull,
    gfull,
    ufull,
    dfull,
    proj,
    after,
    normed,
    xn,
    hid,
    keep,
    pcs,
    pcr,
    raws,
    rawr,
    nbs,
    nbr,
    ffn,
    residual_ref,
    own_sem,
    halo_send,
    halo_recv,
    z_send,
    z_recv,
    y_send,
    y_recv,
    ag_send,
    ag_recv,
    pc_send,
    pc_recv,
    raw_send,
    raw_recv,
    nb_send,
    nb_recv,
):
    n_sp, n_tp = lax.axis_size("sp"), lax.axis_size("tp")
    n_x, reach = n_tp // 2, n_sp // 2
    g = lax.axis_index("grp")
    s = lax.axis_index("sp")
    t = lax.axis_index("tp")
    core = lax.rem(t, 2)
    other = 1 - core
    x = t // 2
    length = query_ref.shape[0]
    rows, dim = residual_hbm.shape
    half = n_x * rows
    depth = gate_ref.shape[0]
    third = gate_ref.shape[1] // 3
    width = down_ref.shape[1]

    z_next = {"sp": lax.rem(s + 1, n_sp)}
    z_prev = {"sp": lax.rem(s + n_sp - 1, n_sp)}
    z_to = (z_next, z_prev)
    x_next = {"tp": lax.rem(t + 2, n_tp)}
    x_prev = {"tp": lax.rem(t + n_tp - 2, n_tp)}
    partner = {"tp": t + 1 - 2 * core}
    odd = lax.rem(g, 2)
    y_pair = {"grp": g + 1 - 2 * odd}
    mine, theirs = 2 * odd, 2 - 2 * odd

    barrier = pltpu.get_barrier_semaphore()
    for device in (z_next, z_prev, x_next, x_prev, partner, y_pair):
        pl.semaphore_signal(barrier, inc=1, device_id=device, device_id_type=MESH)
    pl.semaphore_wait(barrier, 6)

    def send(src, dst, ssem, rsem, device):
        pltpu.make_async_remote_copy(
            src_ref=src, dst_ref=dst, send_sem=ssem, recv_sem=rsem, device_id=device, device_id_type=MESH
        ).start()

    def sent(size, ssem):
        pltpu.make_async_remote_copy(
            src_ref=size, dst_ref=size, send_sem=ssem, recv_sem=ssem, device_id=partner, device_id_type=MESH
        ).wait_send()

    def landed(dst, ssem, rsem, device):
        pltpu.make_async_remote_copy(
            src_ref=dst, dst_ref=dst, send_sem=ssem, recv_sem=rsem, device_id=device, device_id_type=MESH
        ).wait_recv()

    fulls = {"gate": gfull, "up": ufull}
    owns = {"gate": gate_ref, "up": up_ref}
    names = ("gate", "up", "down", "out")
    z_base, z_at = {}, 0
    for name in names:
        z_base[name] = z_at
        z_at += reach * 2 * PARTS[name]

    def place(name, j, way, part, h):
        if name in fulls:
            origin = lax.rem(s + n_sp - j, n_sp) if way == 0 else lax.rem(s + j, n_sp)
            size = depth // PARTS[name]
            at = pl.multiple_of(origin * depth + h * size, size)
            return fulls[name].at[part, pl.ds(at, size), :]
        slot, side = (0, 1) if j == reach else (j, way)
        if name == "out":
            size = out_weight_ref.shape[0] // 2
            return ofull.at[slot, side, pl.ds(part * size, size), :]
        size = third // PARTS[name]
        at = pl.multiple_of(part * third + h * size, size)
        return dfull.at[slot, side, pl.ds(at, size), :]

    def dest(name, j, way, part, h):
        return place(name, j if name in fulls else j + 1, way, part, h)

    def own_piece(name, part, h):
        if name in fulls:
            size = depth // PARTS[name]
            lanes = pl.ds(pl.multiple_of(part * third, third), third)
            return owns[name].at[pl.ds(h * size, size), lanes]
        if name == "out":
            size = out_weight_ref.shape[0] // 2
            return out_weight_ref.at[pl.ds(part * size, size), :]
        size = third // PARTS[name]
        return down_ref.at[pl.ds(pl.multiple_of(part * third + h * size, size), size), :]

    def z_sem(name, j, kind, h):
        return z_recv.at[z_base[name] + (j * 2 + kind) * PARTS[name] + h]

    def y_sem(name, j):
        return y_recv.at[names.index(name) if name in fulls else 1 + j]

    def travels(j, way, kind):
        return j < reach - 1 or (j == reach - 1 and way == kind)

    def part_of(name, kind):
        if name == "out":
            return kind
        return mine if kind == 0 else 1

    def start_own(name, kind):
        part = part_of(name, kind)
        for h in range(PARTS[name]):
            for way in range(2):
                there = dest(name, 0, way, part, h)
                which = z_send.at[names.index(name)]
                send(own_piece(name, part, h), there, which, z_sem(name, 0, kind, h), z_to[way])

    def step(name, kind, j):
        part = part_of(name, kind)
        which = names.index(name)
        ends = [way for way in range(2) if travels(j - 1, way, kind)]
        for h in range(PARTS[name]):
            landed(as_many(name, len(ends)), z_send.at[which], z_sem(name, j - 1, kind, h), z_next)
            for way in ends:
                here = place(name, j, way, part, h)
                if j < reach and travels(j, way, kind):
                    there = dest(name, j, way, part, h)
                    send(here, there, z_send.at[which], z_sem(name, j, kind, h), z_to[way])
                if kind == 0 and name != "out":
                    send(here, here, y_send.at[which], y_sem(name, j), y_pair)

    def as_many(name, count):
        if name in fulls:
            return fulls[name].at[0, pl.ds(0, count * (depth // PARTS[name])), :]
        if name == "out":
            return ofull.at[0, 0, pl.ds(0, count * (out_weight_ref.shape[0] // 2)), :]
        return dfull.at[0, 0, pl.ds(0, count * (third // PARTS[name])), :]

    def steps_of(r):
        todo = []
        for name, kind, lag in STREAMS:
            if 1 <= r - lag <= reach:
                todo.append(functools.partial(step, name, kind, r - lag))
        for name, kind, lag in STREAMS:
            if 0 < lag == r:
                todo.append(functools.partial(start_own, name, kind))
        return todo

    rounds = max(lag for _, _, lag in STREAMS) + reach
    waiting = [(r, todo) for r in range(1, rounds + 1) for todo in steps_of(r)]

    def serve(count):
        for _ in range(min(count, len(waiting))):
            waiting.pop(0)[1]()

    def serve_through(r):
        while waiting and waiting[0][0] <= r:
            waiting.pop(0)[1]()

    def serve_until(name, j, kind=1):
        while any(
            todo.func is step and todo.args[0] == name and todo.args[1] <= kind and todo.args[2] <= j
            for _, todo in waiting
        ):
            waiting.pop(0)[1]()

    def swapped(name, j=1):
        which = names.index(name)
        if name in fulls:
            size = fulls[name].at[0, pl.ds(0, (n_sp - 1) * depth), :]
        else:
            size = dfull.at[0, 0, pl.ds(0, (2 if j < reach else 1) * third), :]
        landed(size, y_send.at[which], y_sem(name, j), y_pair)

    order = [*range(1, reach), 0]
    ways = ((x_next, x_prev), (x_prev, x_next))

    def origin_of(slot, side):
        if slot == 0:
            return s if side == 0 else lax.rem(s + reach, n_sp)
        return lax.rem(s + n_sp - slot, n_sp) if side == 0 else lax.rem(s + slot, n_sp)

    def summing(which, product, result):
        def slot_of(i):
            return which * reach + i

        def make(i):
            m = slot_of(i)
            pcs[m] = product(order[i], pl.multiple_of(other * half, half)).astype(bf16)
            send(pcs.at[m], pcr.at[m], pc_send.at[0], pc_recv.at[i], partner)
            keep[i] = product(order[i], pl.multiple_of(core * half, half))

        def chip_rows(i, xx, side):
            at = pl.multiple_of(lax.rem(xx + n_x, n_x) * rows, rows)
            lanes = slice(side * width, (side + 1) * width)
            return keep[i, pl.ds(at, rows), lanes] + pcr[slot_of(i), pl.ds(at, rows), lanes].astype(f32)

        def spread(i):
            m = slot_of(i)
            landed(pcr.at[m], pc_send.at[0], pc_recv.at[i], partner)
            for side in range(2):
                forth, back = ways[side]
                sign = 1 - 2 * side
                raws[m, side] = chip_rows(i, x + 2, side).astype(bf16)
                send(raws.at[m, side], rawr.at[m, side], raw_send.at[0], raw_recv.at[i], forth)
                nbs[m, side, 1] = chip_rows(i, x - sign, side).astype(bf16)
                send(nbs.at[m, side, 1], nbr.at[m, side, 1], nb_send.at[0], nb_recv.at[i], back)

        def pass_on(i):
            m = slot_of(i)
            landed(rawr.at[m], raw_send.at[0], raw_recv.at[i], x_next)
            for side in range(2):
                forth, back = ways[side]
                sign = 1 - 2 * side
                nbs[m, side, 0] = (chip_rows(i, x + sign, side) + rawr[m, side].astype(f32)).astype(bf16)
                send(nbs.at[m, side, 0], nbr.at[m, side, 0], nb_send.at[0], nb_recv.at[i], forth)

        def collect(i):
            m = slot_of(i)
            landed(nbr.at[m], nb_send.at[0], nb_recv.at[i], x_next)
            for side in range(2):
                total = chip_rows(i, x, side) + nbr[m, side, 0].astype(f32)
                result[origin_of(order[i], side)] = total + nbr[m, side, 1].astype(f32)

        return make, spread, pass_on, collect

    def block_of(c, xx):
        return pl.multiple_of((c * n_x + lax.rem(xx + n_x, n_x)) * rows, rows)

    blocks = length // WINDOW
    docs[0] = doc_ref[blocks - 1 : blocks, :]
    for i, (src, dst) in enumerate(((key_ref, keys), (value_ref, values))):
        send(
            src.at[:, pl.ds(length - WINDOW, WINDOW)],
            dst.at[:, pl.ds(0, WINDOW)],
            halo_send.at[i],
            halo_recv.at[i],
            z_next,
        )
    send(docs.at[0], docs.at[1], halo_send.at[2], halo_recv.at[2], z_next)
    for name, kind, lag in STREAMS:
        if lag == 0:
            start_own(name, kind)
    for name in fulls:
        at = pl.multiple_of(s * depth, depth)
        for k in range(3):
            mine_rows = fulls[name].at[k, pl.ds(at, depth), :]
            pltpu.make_async_copy(owns[name].at[:, pl.ds(k * third, third)], mine_rows, own_sem.at[0]).start()
    pltpu.make_async_copy(down_ref, dfull.at[0, 0], own_sem.at[0]).start()
    pltpu.make_async_copy(out_weight_ref, ofull.at[0, 0], own_sem.at[0]).start()
    pltpu.make_async_copy(residual_hbm, residual_ref, own_sem.at[1]).start()
    keys[:, WINDOW:] = key_ref[...]
    values[:, WINDOW:] = value_ref[...]

    def column(row):
        return jnp.transpose(jnp.broadcast_to(row, (WINDOW, WINDOW)))

    def attend(b):
        first = b * WINDOW
        query = query_ref[first : first + WINDOW, :]
        query = jnp.concatenate([query[:, :HEAD_DIM], query[:, HEAD_DIM:]], axis=0)
        window = slice(first, first + 2 * WINDOW)
        scores = jnp.dot(query, keys[:, window], preferred_element_type=f32) * HEAD_DIM ** (-0.5)
        at_row = lax.broadcasted_iota(jnp.int32, (WINDOW, 2 * WINDOW), 0)
        at_col = lax.broadcasted_iota(jnp.int32, (WINDOW, 2 * WINDOW), 1)
        distance = at_row - at_col + WINDOW
        place_of_key = s * length + (first - WINDOW) + at_col
        own_doc = doc_ref[b : b + 1, :]
        mine_doc = column(own_doc)
        mine_doc = jnp.concatenate([mine_doc, mine_doc], axis=1)
        earlier = docs[1] if b == 0 else doc_ref[b - 1 : b, :]
        valid = (distance >= 0) & (distance < WINDOW) & (place_of_key >= 0)
        valid = valid & (mine_doc == jnp.concatenate([earlier, own_doc], axis=1))
        bias = jnp.where(valid, 0.0, masked_value)
        bias = jnp.concatenate([bias, bias], axis=0)
        scores = jnp.where(bias < 0.0, masked_value, scores)
        head = lax.broadcasted_iota(jnp.int32, (2 * WINDOW, 1), 0)
        sinks = jnp.where(head < WINDOW, sink_ref[0], sink_ref[1])
        top = jnp.maximum(jnp.max(scores, axis=-1, keepdims=True), sinks)
        weight = jnp.exp(scores - top)
        denom = jnp.sum(weight, axis=-1, keepdims=True) + jnp.exp(sinks - top)
        summed = lax.dot_general(
            weight.astype(bf16),
            values[:, window],
            (((1,), (1,)), ((), ())),
            preferred_element_type=f32,
        ) / denom
        mixed[first : first + WINDOW, :] = jnp.concatenate(
            [summed[:WINDOW], summed[WINDOW:]], axis=1
        ).astype(bf16)

    for b in range(1, blocks):
        attend(b)
    serve_until("out", 1)
    landed(keys.at[:, pl.ds(0, WINDOW)], halo_send.at[0], halo_recv.at[0], z_prev)
    landed(values.at[:, pl.ds(0, WINDOW)], halo_send.at[1], halo_recv.at[1], z_prev)
    landed(docs.at[1], halo_send.at[2], halo_recv.at[2], z_prev)
    attend(0)
    for d in range(n_tp):
        u = (d % 2) * n_x + d // 2
        heads[u * rows : (u + 1) * rows, :] = mixed[d * rows : (d + 1) * rows, :]
    arrived = gfull.at[0, pl.ds(0, 9 * depth + depth // 2), :]
    pltpu.make_async_copy(arrived, arrived, own_sem.at[0]).wait()
    pltpu.make_async_copy(residual_hbm, residual_ref, own_sem.at[1]).wait()

    def project(slot, at):
        right = jnp.concatenate([ofull[slot, side] for side in range(2)], axis=1)
        return jnp.dot(heads[pl.ds(at, half), :], right, preferred_element_type=f32)

    make, spread, pass_on, collect = summing(0, project, proj)
    for i in range(reach):
        serve_until("out", i + 1)
        make(i)
        if i >= 1:
            pass_on(i - 1)
        if i >= 2:
            collect(i - 2)
        serve(SERVE_RS[2] if i == reach - 1 else 1)
        spread(i)
        if i < reach - 1:
            serve_through(i + 1)
    serve(SERVE_RS[0])
    pass_on(reach - 1)
    collect(reach - 2)
    serve(SERVE_RS[1])
    collect(reach - 1)

    def scale_of(squares):
        return lax.rsqrt(squares / dim + epsilon)

    def normalise():
        squares = None
        for n in range(n_sp):
            v = proj[n].astype(bf16).astype(f32)
            part = jnp.sum(v * v, axis=-1, keepdims=True)
            squares = part if squares is None else squares + part
        scale = scale_of(squares)
        squares = None
        for n in range(n_sp):
            lanes = slice(n * width, (n + 1) * width)
            v = proj[n].astype(bf16).astype(f32)
            v = residual_ref[:, lanes].astype(f32) + v * scale * gain_mixed_ref[:, lanes]
            v = v.astype(bf16)
            after[:, lanes] = v
            v = v.astype(f32)
            part = jnp.sum(v * v, axis=-1, keepdims=True)
            squares = part if squares is None else squares + part
        scale = scale_of(squares)
        for n in range(n_sp):
            lanes = slice(n * width, (n + 1) * width)
            v = after[:, lanes].astype(f32)
            normed[:, lanes] = (v * scale * gain_before_ref[:, lanes]).astype(bf16)

    normalise()

    h_rows = rows // 2
    ag_at = {}

    def row_part(c, xx, h):
        return xn.at[pl.ds(pl.multiple_of(block_of(c, xx) + h * h_rows, h_rows), h_rows), :]

    def ag_send_to(key, src, dst, device):
        if key not in ag_at:
            ag_at[key] = len(ag_at)
        send(src, dst, ag_send.at[0], ag_recv.at[ag_at[key]], device)

    def ag_wait(key, dst):
        landed(dst, ag_send.at[0], ag_recv.at[ag_at[key]], partner)

    for h in range(2):
        src = normed.at[pl.ds(h * h_rows, h_rows), :]
        ag_send_to(("next", h), src, row_part(core, x, h), x_next)
        src = normed.at[pl.ds((1 - h) * h_rows, h_rows), :]
        ag_send_to(("prev", 1 - h), src, row_part(core, x, 1 - h), x_prev)
        src = normed.at[pl.ds(h * h_rows, h_rows), :]
        ag_send_to("partner", src, row_part(core, x, h), partner)
    xn[pl.ds(block_of(core, x), rows), :] = normed[...]

    def relay(h):
        for key, hh, xx, far, to in (("next", h, x - 1, 0, x_next), ("prev", 1 - h, x + 1, 1, x_prev)):
            here = row_part(core, xx, hh)
            ag_wait((key, hh), here)
            if hh == far:
                ag_send_to(("far", hh), here, here, to)
            ag_send_to("partner", here, here, partner)

    def relay_far(h):
        here = row_part(core, x + 2, h)
        ag_wait(("far", h), here)
        ag_send_to("partner", here, here, partner)

    serve(SERVE_AG[0])
    relay(0)
    serve(SERVE_AG[1])
    relay(1)
    serve(SERVE_AG[2])
    relay_far(0)
    relay_far(1)
    serve(SERVE_AG[3])
    ag_wait("partner", xn.at[pl.ds(block_of(other, 0), half), :])

    def units(k, b):
        piece = xn[b * half : (b + 1) * half, :]
        gate = jnp.dot(piece, gfull[k], preferred_element_type=f32)
        up = jnp.dot(piece, ufull[k], preferred_element_type=f32)
        hid[k, b * half : (b + 1) * half, :] = (gate / (1.0 + jnp.exp(-gate)) * up).astype(bf16)

    for turn, k in enumerate((mine, theirs, 1)):
        for name in fulls:
            if turn == 1:
                swapped(name)
            else:
                serve_until(name, reach, turn // 2)
        for b in range(2):
            units(k, b)
            serve(SERVE_UNITS)

    def lower(slot, at):
        total = None
        for k in range(3):
            right = jnp.concatenate(
                [dfull[slot, side, k * third : (k + 1) * third, :] for side in range(2)], axis=1
            )
            term = jnp.dot(hid[k, pl.ds(at, half), :], right, preferred_element_type=f32)
            total = term if total is None else total + term
        return total

    make, spread, pass_on, collect = summing(1, lower, ffn)
    for i in range(reach):
        if i >= 1:
            spread(i - 1)
        if i >= 3:
            pass_on(i - 3)
        if i >= 5:
            collect(i - 5)
        serve_until("down", i + 1)
        swapped("down", i + 1)
        make(i)
        serve(1)
    pass_on(reach - 3)
    collect(reach - 5)
    spread(reach - 1)
    pass_on(reach - 2)
    collect(reach - 4)
    collect(reach - 3)
    pass_on(reach - 1)
    collect(reach - 2)
    collect(reach - 1)

    def finish():
        squares = None
        for n in range(n_sp):
            v = ffn[n].astype(bf16).astype(f32)
            part = jnp.sum(v * v, axis=-1, keepdims=True)
            squares = part if squares is None else squares + part
        scale = scale_of(squares)
        for n in range(n_sp):
            lanes = slice(n * width, (n + 1) * width)
            v = ffn[n].astype(bf16).astype(f32)
            out_ref[:, lanes] = (
                after[:, lanes].astype(f32) + 0.5 * (v * scale * gain_after_ref[:, lanes])
            ).astype(bf16)

    finish()

    def drain():
        trips = n_sp - 1
        shard = gfull.at[pl.ds(0, 2), pl.ds(0, trips * depth), :]
        swap = gfull.at[0, pl.ds(0, trips * depth), :]
        for i, name in enumerate(names):
            if name == "out":
                sent(gfull.at[0, pl.ds(0, trips * depth // 2), :], z_send.at[i])
            else:
                sent(shard, z_send.at[i])
                sent(swap, y_send.at[i])
        sent(xn.at[pl.ds(0, length - rows), :], ag_send.at[0])
        sent(pcs, pc_send.at[0])
        sent(raws, raw_send.at[0])
        sent(nbs, nb_send.at[0])
        tail = pl.ds(0, WINDOW)
        sent(keys.at[:, tail], halo_send.at[0])
        sent(values.at[:, tail], halo_send.at[1])
        sent(docs.at[0], halo_send.at[2])

    drain()


def per_device(
    queries,
    key_rows,
    value_rows,
    doc_ids,
    sink_logits,
    out_weight,
    residual,
    gain_mixed,
    gain_before,
    gain_after,
    gate_weight,
    up_weight,
    down_weight,
):
    n_sp, n_tp = lax.axis_size("sp"), lax.axis_size("tp")
    n_x, reach = n_tp // 2, n_sp // 2
    length = queries.shape[0]
    rows, dim = residual.shape
    depth, hidden = gate_weight.shape
    width = down_weight.shape[1]
    third = hidden // 3
    half = n_x * rows
    vmem = pl.BlockSpec(memory_space=pltpu.VMEM)
    smem = pl.BlockSpec(memory_space=pltpu.SMEM)
    hbm = pl.BlockSpec(memory_space=pl.ANY)
    dma = pltpu.SemaphoreType.DMA
    pieces = sum(PARTS.values())
    return pl.pallas_call(
        kernel,
        out_shape=jax.ShapeDtypeStruct((rows, dim), bf16),
        in_specs=[vmem] * 4 + [smem, hbm] + [vmem] * 3 + [hbm] * 4,
        out_specs=vmem,
        scratch_shapes=[
            pltpu.VMEM((key_rows.shape[1], length + WINDOW), bf16),
            pltpu.VMEM((value_rows.shape[1], length + WINDOW), bf16),
            pltpu.VMEM((2, 1, WINDOW), jnp.int32),
            pltpu.VMEM(queries.shape, bf16),
            pltpu.VMEM(queries.shape, bf16),
            pltpu.VMEM((reach, 2, *out_weight.shape), bf16),
            pltpu.VMEM((3, n_sp * depth, third), bf16),
            pltpu.VMEM((3, n_sp * depth, third), bf16),
            pltpu.VMEM((reach, 2, hidden, width), bf16),
            pltpu.VMEM((n_sp, rows, width), f32),
            pltpu.VMEM((rows, dim), bf16),
            pltpu.VMEM((rows, dim), bf16),
            pltpu.VMEM((length, dim), bf16),
            pltpu.VMEM((3, length, third), bf16),
            pltpu.VMEM((reach, half, 2 * width), f32),
            pltpu.VMEM((2 * reach, half, 2 * width), bf16),
            pltpu.VMEM((2 * reach, half, 2 * width), bf16),
            pltpu.VMEM((2 * reach, 2, rows, width), bf16),
            pltpu.VMEM((2 * reach, 2, rows, width), bf16),
            pltpu.VMEM((2 * reach, 2, 2, rows, width), bf16),
            pltpu.VMEM((2 * reach, 2, 2, rows, width), bf16),
            pltpu.VMEM((n_sp, rows, width), f32),
            pltpu.VMEM((rows, dim), bf16),
            dma((2,)),
            dma((3,)),
            dma((3,)),
            dma((4,)),
            dma((2 * reach * pieces,)),
            dma((3,)),
            dma((2 + reach,)),
            dma((1,)),
            dma((7,)),
            dma((1,)),
            dma((reach,)),
            dma((1,)),
            dma((reach,)),
            dma((1,)),
            dma((reach,)),
        ],
        compiler_params=pltpu.CompilerParams(
            collective_id=0, has_side_effects=True, vmem_limit_bytes=60 * 1024 * 1024
        ),
    )(
        queries,
        key_rows.T,
        value_rows.T,
        doc_ids.reshape(-1, WINDOW),
        sink_logits,
        residual,
        gain_mixed.reshape(1, -1),
        gain_before.reshape(1, -1),
        gain_after.reshape(1, -1),
        out_weight,
        gate_weight,
        up_weight,
        down_weight,
    )


def solution(mesh):
    return jax.shard_map(
        per_device,
        mesh=mesh,
        in_specs=(
            P(("grp", "sp"), "tp"),
            P(("grp", "sp"), "tp"),
            P(("grp", "sp"), "tp"),
            P(("grp", "sp")),
            P("tp"),
            P("tp", "sp"),
            P(("grp", "sp", "tp"), None),
            P(),
            P(),
            P(),
            P("sp", "tp"),
            P("sp", "tp"),
            P("tp", "sp"),
        ),
        out_specs=P(("grp", "sp", "tp"), None),
        check_vma=False,
    )
```

```python
import functools

import jax
import jax.numpy as jnp
from jax import lax
from jax.experimental import pallas as pl
from jax.experimental.pallas import tpu as pltpu
from jax.sharding import PartitionSpec as P

HEAD_DIM = 64
WINDOW = 128
epsilon = 1e-06
masked_value = -1e30
MESH = pl.DeviceIdType.MESH
f32 = jnp.float32
bf16 = jnp.bfloat16

PARTS = {"gate": 2, "up": 2, "down": 2, "out": 1}
STREAMS = (
    ("out", 0, 0),
    ("out", 1, 0),
    ("gate", 0, 0),
    ("gate", 1, 4),
    ("up", 0, 0),
    ("up", 1, 5),
    ("down", 0, 7),
    ("down", 1, 7),
)
SERVE_RS = (2, 2, 1)
SERVE_AG = (5, 3, 3, 2)
SERVE_UNITS = 1


def kernel(
    query_hbm,
    key_hbm,
    value_hbm,
    doc_hbm,
    sink_hbm,
    residual_hbm,
    gain_mixed_hbm,
    gain_before_hbm,
    gain_after_hbm,
    out_weight_ref,
    gate_ref,
    up_ref,
    down_ref,
    out_ref,
    keys,
    values,
    docs,
    mixed,
    heads,
    ofull,
    gfull,
    ufull,
    dfull,
    proj,
    after,
    normed,
    xn,
    hid,
    keep,
    pcs,
    pcr,
    raws,
    rawr,
    nbs,
    nbr,
    ffn,
    residual_ref,
    query_ref,
    doc_ref,
    sink_ref,
    gain_mixed_ref,
    gain_before_ref,
    gain_after_ref,
    own_sem,
    halo_send,
    halo_recv,
    z_send,
    z_recv,
    y_send,
    y_recv,
    ag_send,
    ag_recv,
    pc_send,
    pc_recv,
    raw_send,
    raw_recv,
    nb_send,
    nb_recv,
):
    n_sp, n_tp = lax.axis_size("sp"), lax.axis_size("tp")
    n_x, reach = n_tp // 2, n_sp // 2
    g = lax.axis_index("grp")
    s = lax.axis_index("sp")
    t = lax.axis_index("tp")
    core = lax.rem(t, 2)
    other = 1 - core
    x = t // 2
    length = query_hbm.shape[0]
    rows, dim = residual_hbm.shape
    half = n_x * rows
    depth = gate_ref.shape[0]
    third = gate_ref.shape[1] // 3
    width = down_ref.shape[1]

    z_next = {"sp": lax.rem(s + 1, n_sp)}
    z_prev = {"sp": lax.rem(s + n_sp - 1, n_sp)}
    z_to = (z_next, z_prev)
    x_next = {"tp": lax.rem(t + 2, n_tp)}
    x_prev = {"tp": lax.rem(t + n_tp - 2, n_tp)}
    partner = {"tp": t + 1 - 2 * core}
    odd = lax.rem(g, 2)
    y_pair = {"grp": g + 1 - 2 * odd}
    mine, theirs = 2 * odd, 2 - 2 * odd

    fetches = {
        "query": (query_hbm, query_ref),
        "key": (key_hbm, keys.at[:, pl.ds(WINDOW, length)]),
        "value": (value_hbm, values.at[:, pl.ds(WINDOW, length)]),
        "doc": (doc_hbm, doc_ref),
        "sink": (sink_hbm, sink_ref),
        "residual": (residual_hbm, residual_ref),
        "gain_mixed": (gain_mixed_hbm, gain_mixed_ref),
        "gain_before": (gain_before_hbm, gain_before_ref),
        "gain_after": (gain_after_hbm, gain_after_ref),
    }

    def fetch(name):
        src, dst = fetches[name]
        return pltpu.make_async_copy(src, dst, own_sem.at[1 + list(fetches).index(name)])

    barrier = pltpu.get_barrier_semaphore()
    for device in (z_next, z_prev, x_next, x_prev, partner, y_pair):
        pl.semaphore_signal(barrier, inc=1, device_id=device, device_id_type=MESH)
    for name in fetches:
        fetch(name).start()
    pl.semaphore_wait(barrier, 6)

    def send(src, dst, ssem, rsem, device):
        pltpu.make_async_remote_copy(
            src_ref=src, dst_ref=dst, send_sem=ssem, recv_sem=rsem, device_id=device, device_id_type=MESH
        ).start()

    def sent(size, ssem):
        pltpu.make_async_remote_copy(
            src_ref=size, dst_ref=size, send_sem=ssem, recv_sem=ssem, device_id=partner, device_id_type=MESH
        ).wait_send()

    def landed(dst, ssem, rsem, device):
        pltpu.make_async_remote_copy(
            src_ref=dst, dst_ref=dst, send_sem=ssem, recv_sem=rsem, device_id=device, device_id_type=MESH
        ).wait_recv()

    fulls = {"gate": gfull, "up": ufull}
    owns = {"gate": gate_ref, "up": up_ref}
    names = ("gate", "up", "down", "out")
    z_base, z_at = {}, 0
    for name in names:
        z_base[name] = z_at
        z_at += reach * 2 * PARTS[name]

    def place(name, j, way, part, h):
        if name in fulls:
            origin = lax.rem(s + n_sp - j, n_sp) if way == 0 else lax.rem(s + j, n_sp)
            size = depth // PARTS[name]
            at = pl.multiple_of(origin * depth + h * size, size)
            return fulls[name].at[part, pl.ds(at, size), :]
        slot, side = (0, 1) if j == reach else (j, way)
        if name == "out":
            size = out_weight_ref.shape[0] // 2
            return ofull.at[slot, side, pl.ds(part * size, size), :]
        size = third // PARTS[name]
        at = pl.multiple_of(part * third + h * size, size)
        return dfull.at[slot, side, pl.ds(at, size), :]

    def dest(name, j, way, part, h):
        return place(name, j if name in fulls else j + 1, way, part, h)

    def own_piece(name, part, h):
        if name in fulls:
            size = depth // PARTS[name]
            lanes = pl.ds(pl.multiple_of(part * third, third), third)
            return owns[name].at[pl.ds(h * size, size), lanes]
        if name == "out":
            size = out_weight_ref.shape[0] // 2
            return out_weight_ref.at[pl.ds(part * size, size), :]
        size = third // PARTS[name]
        return down_ref.at[pl.ds(pl.multiple_of(part * third + h * size, size), size), :]

    def z_sem(name, j, kind, h):
        return z_recv.at[z_base[name] + (j * 2 + kind) * PARTS[name] + h]

    def y_sem(name, j):
        return y_recv.at[names.index(name) if name in fulls else 1 + j]

    def travels(j, way, kind):
        return j < reach - 1 or (j == reach - 1 and way == kind)

    def part_of(name, kind):
        if name == "out":
            return kind
        return mine if kind == 0 else 1

    def start_own(name, kind):
        part = part_of(name, kind)
        for h in range(PARTS[name]):
            for way in range(2):
                there = dest(name, 0, way, part, h)
                which = z_send.at[names.index(name)]
                send(own_piece(name, part, h), there, which, z_sem(name, 0, kind, h), z_to[way])

    def step(name, kind, j):
        part = part_of(name, kind)
        which = names.index(name)
        ends = [way for way in range(2) if travels(j - 1, way, kind)]
        for h in range(PARTS[name]):
            landed(as_many(name, len(ends)), z_send.at[which], z_sem(name, j - 1, kind, h), z_next)
            for way in ends:
                here = place(name, j, way, part, h)
                if j < reach and travels(j, way, kind):
                    there = dest(name, j, way, part, h)
                    send(here, there, z_send.at[which], z_sem(name, j, kind, h), z_to[way])
                if kind == 0 and name != "out":
                    send(here, here, y_send.at[which], y_sem(name, j), y_pair)

    def as_many(name, count):
        if name in fulls:
            return fulls[name].at[0, pl.ds(0, count * (depth // PARTS[name])), :]
        if name == "out":
            return ofull.at[0, 0, pl.ds(0, count * (out_weight_ref.shape[0] // 2)), :]
        return dfull.at[0, 0, pl.ds(0, count * (third // PARTS[name])), :]

    def steps_of(r):
        todo = []
        for name, kind, lag in STREAMS:
            if 1 <= r - lag <= reach:
                todo.append(functools.partial(step, name, kind, r - lag))
        for name, kind, lag in STREAMS:
            if 0 < lag == r:
                todo.append(functools.partial(start_own, name, kind))
        return todo

    rounds = max(lag for _, _, lag in STREAMS) + reach
    waiting = [(r, todo) for r in range(1, rounds + 1) for todo in steps_of(r)]

    def serve(count):
        for _ in range(min(count, len(waiting))):
            waiting.pop(0)[1]()

    def serve_through(r):
        while waiting and waiting[0][0] <= r:
            waiting.pop(0)[1]()

    def serve_until(name, j, kind=1):
        while any(
            todo.func is step and todo.args[0] == name and todo.args[1] <= kind and todo.args[2] <= j
            for _, todo in waiting
        ):
            waiting.pop(0)[1]()

    def swapped(name, j=1):
        which = names.index(name)
        if name in fulls:
            size = fulls[name].at[0, pl.ds(0, (n_sp - 1) * depth), :]
        else:
            size = dfull.at[0, 0, pl.ds(0, (2 if j < reach else 1) * third), :]
        landed(size, y_send.at[which], y_sem(name, j), y_pair)

    order = [*range(1, reach), 0]
    ways = ((x_next, x_prev), (x_prev, x_next))

    def origin_of(slot, side):
        if slot == 0:
            return s if side == 0 else lax.rem(s + reach, n_sp)
        return lax.rem(s + n_sp - slot, n_sp) if side == 0 else lax.rem(s + slot, n_sp)

    def summing(which, product, result):
        def slot_of(i):
            return which * reach + i

        def make(i):
            m = slot_of(i)
            pcs[m] = product(order[i], pl.multiple_of(other * half, half)).astype(bf16)
            send(pcs.at[m], pcr.at[m], pc_send.at[0], pc_recv.at[i], partner)
            keep[i] = product(order[i], pl.multiple_of(core * half, half))

        def chip_rows(i, xx, side):
            at = pl.multiple_of(lax.rem(xx + n_x, n_x) * rows, rows)
            lanes = slice(side * width, (side + 1) * width)
            return keep[i, pl.ds(at, rows), lanes] + pcr[slot_of(i), pl.ds(at, rows), lanes].astype(f32)

        def spread(i):
            m = slot_of(i)
            landed(pcr.at[m], pc_send.at[0], pc_recv.at[i], partner)
            for side in range(2):
                forth, back = ways[side]
                sign = 1 - 2 * side
                raws[m, side] = chip_rows(i, x + 2, side).astype(bf16)
                send(raws.at[m, side], rawr.at[m, side], raw_send.at[0], raw_recv.at[i], forth)
                nbs[m, side, 1] = chip_rows(i, x - sign, side).astype(bf16)
                send(nbs.at[m, side, 1], nbr.at[m, side, 1], nb_send.at[0], nb_recv.at[i], back)

        def pass_on(i):
            m = slot_of(i)
            landed(rawr.at[m], raw_send.at[0], raw_recv.at[i], x_next)
            for side in range(2):
                forth, back = ways[side]
                sign = 1 - 2 * side
                nbs[m, side, 0] = (chip_rows(i, x + sign, side) + rawr[m, side].astype(f32)).astype(bf16)
                send(nbs.at[m, side, 0], nbr.at[m, side, 0], nb_send.at[0], nb_recv.at[i], forth)

        def collect(i):
            m = slot_of(i)
            landed(nbr.at[m], nb_send.at[0], nb_recv.at[i], x_next)
            for side in range(2):
                total = chip_rows(i, x, side) + nbr[m, side, 0].astype(f32)
                result[origin_of(order[i], side)] = total + nbr[m, side, 1].astype(f32)

        return make, spread, pass_on, collect

    def block_of(c, xx):
        return pl.multiple_of((c * n_x + lax.rem(xx + n_x, n_x)) * rows, rows)

    blocks = length // WINDOW
    for i, (src, dst) in enumerate(((key_hbm, keys), (value_hbm, values))):
        send(
            src.at[:, pl.ds(length - WINDOW, WINDOW)],
            dst.at[:, pl.ds(0, WINDOW)],
            halo_send.at[i],
            halo_recv.at[i],
            z_next,
        )
    for name, kind, lag in STREAMS:
        if lag == 0 and name == "out":
            start_own(name, kind)
    fetch("doc").wait()
    docs[0] = doc_ref[blocks - 1 : blocks, :]
    send(docs.at[0], docs.at[1], halo_send.at[2], halo_recv.at[2], z_next)
    for name, kind, lag in STREAMS:
        if lag == 0 and name != "out":
            start_own(name, kind)
    for name in fulls:
        at = pl.multiple_of(s * depth, depth)
        for k in range(3):
            mine_rows = fulls[name].at[k, pl.ds(at, depth), :]
            pltpu.make_async_copy(owns[name].at[:, pl.ds(k * third, third)], mine_rows, own_sem.at[0]).start()
    pltpu.make_async_copy(down_ref, dfull.at[0, 0], own_sem.at[0]).start()
    pltpu.make_async_copy(out_weight_ref, ofull.at[0, 0], own_sem.at[0]).start()
    for name in ("query", "key", "value", "sink"):
        fetch(name).wait()

    def column(row):
        return jnp.transpose(jnp.broadcast_to(row, (WINDOW, WINDOW)))

    def attend(b):
        first = b * WINDOW
        query = query_ref[first : first + WINDOW, :]
        query = jnp.concatenate([query[:, :HEAD_DIM], query[:, HEAD_DIM:]], axis=0)
        window = slice(first, first + 2 * WINDOW)
        scores = jnp.dot(query, keys[:, window], preferred_element_type=f32) * HEAD_DIM ** (-0.5)
        at_row = lax.broadcasted_iota(jnp.int32, (WINDOW, 2 * WINDOW), 0)
        at_col = lax.broadcasted_iota(jnp.int32, (WINDOW, 2 * WINDOW), 1)
        distance = at_row - at_col + WINDOW
        place_of_key = s * length + (first - WINDOW) + at_col
        own_doc = doc_ref[b : b + 1, :]
        mine_doc = column(own_doc)
        mine_doc = jnp.concatenate([mine_doc, mine_doc], axis=1)
        earlier = docs[1] if b == 0 else doc_ref[b - 1 : b, :]
        valid = (distance >= 0) & (distance < WINDOW) & (place_of_key >= 0)
        valid = valid & (mine_doc == jnp.concatenate([earlier, own_doc], axis=1))
        bias = jnp.where(valid, 0.0, masked_value)
        bias = jnp.concatenate([bias, bias], axis=0)
        scores = jnp.where(bias < 0.0, masked_value, scores)
        head = lax.broadcasted_iota(jnp.int32, (2 * WINDOW, 1), 0)
        sinks = jnp.where(head < WINDOW, sink_ref[0], sink_ref[1])
        top = jnp.maximum(jnp.max(scores, axis=-1, keepdims=True), sinks)
        weight = jnp.exp(scores - top)
        denom = jnp.sum(weight, axis=-1, keepdims=True) + jnp.exp(sinks - top)
        summed = lax.dot_general(
            weight.astype(bf16),
            values[:, window],
            (((1,), (1,)), ((), ())),
            preferred_element_type=f32,
        ) / denom
        mixed[first : first + WINDOW, :] = jnp.concatenate(
            [summed[:WINDOW], summed[WINDOW:]], axis=1
        ).astype(bf16)

    for b in range(1, blocks):
        attend(b)
    serve_until("out", 1)
    landed(keys.at[:, pl.ds(0, WINDOW)], halo_send.at[0], halo_recv.at[0], z_prev)
    landed(values.at[:, pl.ds(0, WINDOW)], halo_send.at[1], halo_recv.at[1], z_prev)
    landed(docs.at[1], halo_send.at[2], halo_recv.at[2], z_prev)
    attend(0)
    for d in range(n_tp):
        u = (d % 2) * n_x + d // 2
        heads[u * rows : (u + 1) * rows, :] = mixed[d * rows : (d + 1) * rows, :]
    arrived = gfull.at[0, pl.ds(0, 9 * depth + depth // 2), :]
    pltpu.make_async_copy(arrived, arrived, own_sem.at[0]).wait()
    for name in ("residual", "gain_mixed", "gain_before", "gain_after"):
        fetch(name).wait()

    def project(slot, at):
        right = jnp.concatenate([ofull[slot, side] for side in range(2)], axis=1)
        return jnp.dot(heads[pl.ds(at, half), :], right, preferred_element_type=f32)

    make, spread, pass_on, collect = summing(0, project, proj)
    for i in range(reach):
        serve_until("out", i + 1)
        make(i)
        if i >= 1:
            pass_on(i - 1)
        if i >= 2:
            collect(i - 2)
        serve(SERVE_RS[2] if i == reach - 1 else 1)
        spread(i)
        if i < reach - 1:
            serve_through(i + 1)
    serve(SERVE_RS[0])
    pass_on(reach - 1)
    collect(reach - 2)
    serve(SERVE_RS[1])
    collect(reach - 1)

    def scale_of(squares):
        return lax.rsqrt(squares / dim + epsilon)

    def normalise():
        squares = None
        for n in range(n_sp):
            v = proj[n].astype(bf16).astype(f32)
            part = jnp.sum(v * v, axis=-1, keepdims=True)
            squares = part if squares is None else squares + part
        scale = scale_of(squares)
        squares = None
        for n in range(n_sp):
            lanes = slice(n * width, (n + 1) * width)
            v = proj[n].astype(bf16).astype(f32)
            v = residual_ref[:, lanes].astype(f32) + v * scale * gain_mixed_ref[:, lanes]
            v = v.astype(bf16)
            after[:, lanes] = v
            v = v.astype(f32)
            part = jnp.sum(v * v, axis=-1, keepdims=True)
            squares = part if squares is None else squares + part
        scale = scale_of(squares)
        for n in range(n_sp):
            lanes = slice(n * width, (n + 1) * width)
            v = after[:, lanes].astype(f32)
            normed[:, lanes] = (v * scale * gain_before_ref[:, lanes]).astype(bf16)

    normalise()

    h_rows = rows // 2
    ag_at = {}

    def row_part(c, xx, h):
        return xn.at[pl.ds(pl.multiple_of(block_of(c, xx) + h * h_rows, h_rows), h_rows), :]

    def ag_send_to(key, src, dst, device):
        if key not in ag_at:
            ag_at[key] = len(ag_at)
        send(src, dst, ag_send.at[0], ag_recv.at[ag_at[key]], device)

    def ag_wait(key, dst):
        landed(dst, ag_send.at[0], ag_recv.at[ag_at[key]], partner)

    for h in range(2):
        src = normed.at[pl.ds(h * h_rows, h_rows), :]
        ag_send_to(("next", h), src, row_part(core, x, h), x_next)
        src = normed.at[pl.ds((1 - h) * h_rows, h_rows), :]
        ag_send_to(("prev", 1 - h), src, row_part(core, x, 1 - h), x_prev)
        src = normed.at[pl.ds(h * h_rows, h_rows), :]
        ag_send_to("partner", src, row_part(core, x, h), partner)
    xn[pl.ds(block_of(core, x), rows), :] = normed[...]

    def relay(h):
        for key, hh, xx, far, to in (("next", h, x - 1, 0, x_next), ("prev", 1 - h, x + 1, 1, x_prev)):
            here = row_part(core, xx, hh)
            ag_wait((key, hh), here)
            if hh == far:
                ag_send_to(("far", hh), here, here, to)
            ag_send_to("partner", here, here, partner)

    def relay_far(h):
        here = row_part(core, x + 2, h)
        ag_wait(("far", h), here)
        ag_send_to("partner", here, here, partner)

    serve(SERVE_AG[0])
    relay(0)
    serve(SERVE_AG[1])
    relay(1)
    serve(SERVE_AG[2])
    relay_far(0)
    relay_far(1)
    serve(SERVE_AG[3])
    ag_wait("partner", xn.at[pl.ds(block_of(other, 0), half), :])

    def units(k, b):
        piece = xn[b * half : (b + 1) * half, :]
        gate = jnp.dot(piece, gfull[k], preferred_element_type=f32)
        up = jnp.dot(piece, ufull[k], preferred_element_type=f32)
        hid[k, b * half : (b + 1) * half, :] = (gate / (1.0 + jnp.exp(-gate)) * up).astype(bf16)

    for turn, k in enumerate((mine, theirs, 1)):
        for name in fulls:
            if turn == 1:
                swapped(name)
            else:
                serve_until(name, reach, turn // 2)
        for b in range(2):
            units(k, b)
            serve(SERVE_UNITS)

    def lower(slot, at):
        total = None
        for k in range(3):
            right = jnp.concatenate(
                [dfull[slot, side, k * third : (k + 1) * third, :] for side in range(2)], axis=1
            )
            term = jnp.dot(hid[k, pl.ds(at, half), :], right, preferred_element_type=f32)
            total = term if total is None else total + term
        return total

    make, spread, pass_on, collect = summing(1, lower, ffn)
    for i in range(reach):
        if i >= 1:
            spread(i - 1)
        if i >= 3:
            pass_on(i - 3)
        if i >= 5:
            collect(i - 5)
        serve_until("down", i + 1)
        swapped("down", i + 1)
        make(i)
        serve(1)
    pass_on(reach - 3)
    collect(reach - 5)
    spread(reach - 1)
    pass_on(reach - 2)
    collect(reach - 4)
    collect(reach - 3)
    pass_on(reach - 1)
    collect(reach - 2)
    collect(reach - 1)

    def finish():
        squares = None
        for n in range(n_sp):
            v = ffn[n].astype(bf16).astype(f32)
            part = jnp.sum(v * v, axis=-1, keepdims=True)
            squares = part if squares is None else squares + part
        scale = scale_of(squares)
        for n in range(n_sp):
            lanes = slice(n * width, (n + 1) * width)
            v = ffn[n].astype(bf16).astype(f32)
            out_ref[:, lanes] = (
                after[:, lanes].astype(f32) + 0.5 * (v * scale * gain_after_ref[:, lanes])
            ).astype(bf16)

    finish()

    def drain():
        trips = n_sp - 1
        shard = gfull.at[pl.ds(0, 2), pl.ds(0, trips * depth), :]
        swap = gfull.at[0, pl.ds(0, trips * depth), :]
        for i, name in enumerate(names):
            if name == "out":
                sent(gfull.at[0, pl.ds(0, trips * depth // 2), :], z_send.at[i])
            else:
                sent(shard, z_send.at[i])
                sent(swap, y_send.at[i])
        sent(xn.at[pl.ds(0, length - rows), :], ag_send.at[0])
        sent(pcs, pc_send.at[0])
        sent(raws, raw_send.at[0])
        sent(nbs, nb_send.at[0])
        tail = pl.ds(0, WINDOW)
        sent(keys.at[:, tail], halo_send.at[0])
        sent(values.at[:, tail], halo_send.at[1])
        sent(docs.at[0], halo_send.at[2])

    drain()


def per_device(
    queries,
    key_rows,
    value_rows,
    doc_ids,
    sink_logits,
    out_weight,
    residual,
    gain_mixed,
    gain_before,
    gain_after,
    gate_weight,
    up_weight,
    down_weight,
):
    n_sp, n_tp = lax.axis_size("sp"), lax.axis_size("tp")
    n_x, reach = n_tp // 2, n_sp // 2
    length = queries.shape[0]
    rows, dim = residual.shape
    depth, hidden = gate_weight.shape
    width = down_weight.shape[1]
    third = hidden // 3
    half = n_x * rows
    vmem = pl.BlockSpec(memory_space=pltpu.VMEM)
    hbm = pl.BlockSpec(memory_space=pltpu.HBM)
    dma = pltpu.SemaphoreType.DMA
    pieces = sum(PARTS.values())
    return pl.pallas_call(
        kernel,
        out_shape=jax.ShapeDtypeStruct((rows, dim), bf16),
        in_specs=[hbm] * 13,
        out_specs=vmem,
        scratch_shapes=[
            pltpu.VMEM((key_rows.shape[1], length + WINDOW), bf16),
            pltpu.VMEM((value_rows.shape[1], length + WINDOW), bf16),
            pltpu.VMEM((2, 1, WINDOW), jnp.int32),
            pltpu.VMEM(queries.shape, bf16),
            pltpu.VMEM(queries.shape, bf16),
            pltpu.VMEM((reach, 2, *out_weight.shape), bf16),
            pltpu.VMEM((3, n_sp * depth, third), bf16),
            pltpu.VMEM((3, n_sp * depth, third), bf16),
            pltpu.VMEM((reach, 2, hidden, width), bf16),
            pltpu.VMEM((n_sp, rows, width), f32),
            pltpu.VMEM((rows, dim), bf16),
            pltpu.VMEM((rows, dim), bf16),
            pltpu.VMEM((length, dim), bf16),
            pltpu.VMEM((3, length, third), bf16),
            pltpu.VMEM((reach, half, 2 * width), f32),
            pltpu.VMEM((2 * reach, half, 2 * width), bf16),
            pltpu.VMEM((2 * reach, half, 2 * width), bf16),
            pltpu.VMEM((2 * reach, 2, rows, width), bf16),
            pltpu.VMEM((2 * reach, 2, rows, width), bf16),
            pltpu.VMEM((2 * reach, 2, 2, rows, width), bf16),
            pltpu.VMEM((2 * reach, 2, 2, rows, width), bf16),
            pltpu.VMEM((n_sp, rows, width), f32),
            pltpu.VMEM((rows, dim), bf16),
            pltpu.VMEM(queries.shape, bf16),
            pltpu.VMEM((length // WINDOW, WINDOW), jnp.int32),
            pltpu.SMEM(sink_logits.shape, f32),
            pltpu.VMEM((1, dim), f32),
            pltpu.VMEM((1, dim), f32),
            pltpu.VMEM((1, dim), f32),
            dma((10,)),
            dma((3,)),
            dma((3,)),
            dma((4,)),
            dma((2 * reach * pieces,)),
            dma((3,)),
            dma((2 + reach,)),
            dma((1,)),
            dma((7,)),
            dma((1,)),
            dma((reach,)),
            dma((1,)),
            dma((reach,)),
            dma((1,)),
            dma((reach,)),
        ],
        compiler_params=pltpu.CompilerParams(
            collective_id=0, has_side_effects=True, vmem_limit_bytes=44 * 1024 * 1024
        ),
    )(
        *(
            pltpu.with_memory_space_constraint(array, pltpu.HBM)
            for array in (
                queries,
                key_rows.T,
                value_rows.T,
                doc_ids.reshape(-1, WINDOW),
                sink_logits,
                residual,
                gain_mixed.reshape(1, -1),
                gain_before.reshape(1, -1),
                gain_after.reshape(1, -1),
                out_weight,
                gate_weight,
                up_weight,
                down_weight,
            )
        )
    )


def solution(mesh):
    return jax.shard_map(
        per_device,
        mesh=mesh,
        in_specs=(
            P(("grp", "sp"), "tp"),
            P(("grp", "sp"), "tp"),
            P(("grp", "sp"), "tp"),
            P(("grp", "sp")),
            P("tp"),
            P("tp", "sp"),
            P(("grp", "sp", "tp"), None),
            P(),
            P(),
            P(),
            P("sp", "tp"),
            P("sp", "tp"),
            P("tp", "sp"),
        ),
        out_specs=P(("grp", "sp", "tp"), None),
        check_vma=False,
    )
```

```python
import functools

import jax
import jax.numpy as jnp
from jax import lax
from jax.experimental import pallas as pl
from jax.experimental.pallas import tpu as pltpu
from jax.sharding import PartitionSpec as P

HEAD_DIM = 64
WINDOW = 128
epsilon = 1e-06
masked_value = -1e30
MESH = pl.DeviceIdType.MESH
f32 = jnp.float32
bf16 = jnp.bfloat16

PARTS = {"gate": 2, "up": 2, "down": 2, "out": 1}
STREAMS = (
    ("out", 0, 0),
    ("out", 1, 0),
    ("gate", 0, 0),
    ("gate", 1, 4),
    ("up", 0, 0),
    ("up", 1, 5),
    ("down", 0, 7),
    ("down", 1, 7),
)
SERVE_RS = (2, 2, 1)
SERVE_AG = (5, 3, 3, 2)
SERVE_UNITS = 1


def kernel(
    query_hbm,
    key_hbm,
    value_hbm,
    doc_hbm,
    sink_hbm,
    residual_hbm,
    gain_mixed_hbm,
    gain_before_hbm,
    gain_after_hbm,
    out_weight_ref,
    gate_ref,
    up_ref,
    down_ref,
    out_ref,
    keys,
    values,
    docs,
    mixed,
    heads,
    ofull,
    gfull,
    ufull,
    dfull,
    proj,
    after,
    normed,
    xn,
    hid,
    keep,
    pcs,
    pcr,
    raws,
    rawr,
    nbs,
    nbr,
    ffn,
    residual_ref,
    query_ref,
    doc_ref,
    sink_ref,
    gain_mixed_ref,
    gain_before_ref,
    gain_after_ref,
    own_sem,
    halo_send,
    halo_recv,
    z_send,
    z_recv,
    y_send,
    y_recv,
    ag_send,
    ag_recv,
    pc_send,
    pc_recv,
    raw_send,
    raw_recv,
    nb_send,
    nb_recv,
):
    n_sp, n_tp = lax.axis_size("sp"), lax.axis_size("tp")
    n_x, reach = n_tp // 2, n_sp // 2
    g = lax.axis_index("grp")
    s = lax.axis_index("sp")
    t = lax.axis_index("tp")
    core = lax.rem(t, 2)
    other = 1 - core
    x = t // 2
    length = query_hbm.shape[0]
    rows, dim = residual_hbm.shape
    half = n_x * rows
    depth = gate_ref.shape[0]
    third = gate_ref.shape[1] // 3
    width = down_ref.shape[1]

    z_next = {"sp": lax.rem(s + 1, n_sp)}
    z_prev = {"sp": lax.rem(s + n_sp - 1, n_sp)}
    z_to = (z_next, z_prev)
    x_next = {"tp": lax.rem(t + 2, n_tp)}
    x_prev = {"tp": lax.rem(t + n_tp - 2, n_tp)}
    partner = {"tp": t + 1 - 2 * core}
    odd = lax.rem(g, 2)
    y_pair = {"grp": g + 1 - 2 * odd}
    mine, theirs = 2 * odd, 2 - 2 * odd

    fetches = {
        "query": (query_hbm, query_ref),
        "key": (key_hbm, keys.at[:, pl.ds(WINDOW, length)]),
        "value": (value_hbm, values.at[:, pl.ds(WINDOW, length)]),
        "doc": (doc_hbm, doc_ref),
        "sink": (sink_hbm, sink_ref),
        "residual": (residual_hbm, residual_ref),
        "gain_mixed": (gain_mixed_hbm, gain_mixed_ref),
        "gain_before": (gain_before_hbm, gain_before_ref),
        "gain_after": (gain_after_hbm, gain_after_ref),
    }

    def fetch(name):
        src, dst = fetches[name]
        return pltpu.make_async_copy(src, dst, own_sem.at[1 + list(fetches).index(name)])

    barrier = pltpu.get_barrier_semaphore()
    for device in (z_next, z_prev, x_next, x_prev, partner, y_pair):
        pl.semaphore_signal(barrier, inc=1, device_id=device, device_id_type=MESH)
    for name in fetches:
        fetch(name).start()
    pl.semaphore_wait(barrier, 6)

    def send(src, dst, ssem, rsem, device):
        pltpu.make_async_remote_copy(
            src_ref=src, dst_ref=dst, send_sem=ssem, recv_sem=rsem, device_id=device, device_id_type=MESH
        ).start()

    def sent(size, ssem):
        pltpu.make_async_remote_copy(
            src_ref=size, dst_ref=size, send_sem=ssem, recv_sem=ssem, device_id=partner, device_id_type=MESH
        ).wait_send()

    def landed(dst, ssem, rsem, device):
        pltpu.make_async_remote_copy(
            src_ref=dst, dst_ref=dst, send_sem=ssem, recv_sem=rsem, device_id=device, device_id_type=MESH
        ).wait_recv()

    fulls = {"gate": gfull, "up": ufull}
    owns = {"gate": gate_ref, "up": up_ref}
    names = ("gate", "up", "down", "out")
    z_base, z_at = {}, 0
    for name in names:
        z_base[name] = z_at
        z_at += reach * 2 * PARTS[name]

    def place(name, j, way, part, h):
        if name in fulls:
            origin = lax.rem(s + n_sp - j, n_sp) if way == 0 else lax.rem(s + j, n_sp)
            size = depth // PARTS[name]
            at = pl.multiple_of(origin * depth + h * size, size)
            return fulls[name].at[part, pl.ds(at, size), :]
        slot, side = (0, 1) if j == reach else (j, way)
        if name == "out":
            size = out_weight_ref.shape[0] // 2
            return ofull.at[slot, side, pl.ds(part * size, size), :]
        size = third // PARTS[name]
        at = pl.multiple_of(part * third + h * size, size)
        return dfull.at[slot, side, pl.ds(at, size), :]

    def dest(name, j, way, part, h):
        return place(name, j if name in fulls else j + 1, way, part, h)

    def own_piece(name, part, h):
        if name in fulls:
            size = depth // PARTS[name]
            lanes = pl.ds(pl.multiple_of(part * third, third), third)
            return owns[name].at[pl.ds(h * size, size), lanes]
        if name == "out":
            size = out_weight_ref.shape[0] // 2
            return out_weight_ref.at[pl.ds(part * size, size), :]
        size = third // PARTS[name]
        return down_ref.at[pl.ds(pl.multiple_of(part * third + h * size, size), size), :]

    def z_sem(name, j, kind, h):
        return z_recv.at[z_base[name] + (j * 2 + kind) * PARTS[name] + h]

    def y_sem(name, j):
        return y_recv.at[names.index(name) if name in fulls else 1 + j]

    def travels(j, way, kind):
        return j < reach - 1 or (j == reach - 1 and way == kind)

    def part_of(name, kind):
        if name == "out":
            return kind
        return mine if kind == 0 else 1

    def start_own(name, kind):
        part = part_of(name, kind)
        for h in range(PARTS[name]):
            for way in range(2):
                there = dest(name, 0, way, part, h)
                which = z_send.at[names.index(name)]
                send(own_piece(name, part, h), there, which, z_sem(name, 0, kind, h), z_to[way])

    def step(name, kind, j):
        part = part_of(name, kind)
        which = names.index(name)
        ends = [way for way in range(2) if travels(j - 1, way, kind)]
        for h in range(PARTS[name]):
            landed(as_many(name, len(ends)), z_send.at[which], z_sem(name, j - 1, kind, h), z_next)
            for way in ends:
                here = place(name, j, way, part, h)
                if j < reach and travels(j, way, kind):
                    there = dest(name, j, way, part, h)
                    send(here, there, z_send.at[which], z_sem(name, j, kind, h), z_to[way])
                if kind == 0 and name != "out":
                    send(here, here, y_send.at[which], y_sem(name, j), y_pair)

    def as_many(name, count):
        if name in fulls:
            return fulls[name].at[0, pl.ds(0, count * (depth // PARTS[name])), :]
        if name == "out":
            return ofull.at[0, 0, pl.ds(0, count * (out_weight_ref.shape[0] // 2)), :]
        return dfull.at[0, 0, pl.ds(0, count * (third // PARTS[name])), :]

    def steps_of(r):
        todo = []
        for name, kind, lag in STREAMS:
            if 1 <= r - lag <= reach:
                todo.append(functools.partial(step, name, kind, r - lag))
        for name, kind, lag in STREAMS:
            if 0 < lag == r:
                todo.append(functools.partial(start_own, name, kind))
        return todo

    rounds = max(lag for _, _, lag in STREAMS) + reach
    waiting = [(r, todo) for r in range(1, rounds + 1) for todo in steps_of(r)]

    def serve(count):
        for _ in range(min(count, len(waiting))):
            waiting.pop(0)[1]()

    def serve_through(r):
        while waiting and waiting[0][0] <= r:
            waiting.pop(0)[1]()

    def serve_until(name, j, kind=1):
        while any(
            todo.func is step and todo.args[0] == name and todo.args[1] <= kind and todo.args[2] <= j
            for _, todo in waiting
        ):
            waiting.pop(0)[1]()

    def swapped(name, j=1):
        which = names.index(name)
        if name in fulls:
            size = fulls[name].at[0, pl.ds(0, (n_sp - 1) * depth), :]
        else:
            size = dfull.at[0, 0, pl.ds(0, (2 if j < reach else 1) * third), :]
        landed(size, y_send.at[which], y_sem(name, j), y_pair)

    order = [*range(1, reach), 0]
    ways = ((x_next, x_prev), (x_prev, x_next))

    def origin_of(slot, side):
        if slot == 0:
            return s if side == 0 else lax.rem(s + reach, n_sp)
        return lax.rem(s + n_sp - slot, n_sp) if side == 0 else lax.rem(s + slot, n_sp)

    def summing(which, product, result):
        def slot_of(i):
            return which * reach + i

        def make(i):
            m = slot_of(i)
            pcs[m] = product(order[i], pl.multiple_of(other * half, half)).astype(bf16)
            send(pcs.at[m], pcr.at[m], pc_send.at[0], pc_recv.at[i], partner)
            keep[i] = product(order[i], pl.multiple_of(core * half, half))

        def chip_rows(i, xx, side):
            at = pl.multiple_of(lax.rem(xx + n_x, n_x) * rows, rows)
            lanes = slice(side * width, (side + 1) * width)
            return keep[i, pl.ds(at, rows), lanes] + pcr[slot_of(i), pl.ds(at, rows), lanes].astype(f32)

        def spread(i):
            m = slot_of(i)
            landed(pcr.at[m], pc_send.at[0], pc_recv.at[i], partner)
            for side in range(2):
                forth, back = ways[side]
                sign = 1 - 2 * side
                raws[m, side] = chip_rows(i, x + 2, side).astype(bf16)
                send(raws.at[m, side], rawr.at[m, side], raw_send.at[0], raw_recv.at[i], forth)
                nbs[m, side, 1] = chip_rows(i, x - sign, side).astype(bf16)
                send(nbs.at[m, side, 1], nbr.at[m, side, 1], nb_send.at[0], nb_recv.at[i], back)

        def pass_on(i):
            m = slot_of(i)
            landed(rawr.at[m], raw_send.at[0], raw_recv.at[i], x_next)
            for side in range(2):
                forth, back = ways[side]
                sign = 1 - 2 * side
                nbs[m, side, 0] = (chip_rows(i, x + sign, side) + rawr[m, side].astype(f32)).astype(bf16)
                send(nbs.at[m, side, 0], nbr.at[m, side, 0], nb_send.at[0], nb_recv.at[i], forth)

        def collect(i):
            m = slot_of(i)
            landed(nbr.at[m], nb_send.at[0], nb_recv.at[i], x_next)
            for side in range(2):
                total = chip_rows(i, x, side) + nbr[m, side, 0].astype(f32)
                result[origin_of(order[i], side)] = total + nbr[m, side, 1].astype(f32)

        return make, spread, pass_on, collect

    def block_of(c, xx):
        return pl.multiple_of((c * n_x + lax.rem(xx + n_x, n_x)) * rows, rows)

    blocks = length // WINDOW
    for i, (src, dst) in enumerate(((key_hbm, keys), (value_hbm, values))):
        send(
            src.at[:, pl.ds(length - WINDOW, WINDOW)],
            dst.at[:, pl.ds(0, WINDOW)],
            halo_send.at[i],
            halo_recv.at[i],
            z_next,
        )
    for name, kind, lag in STREAMS:
        if lag == 0 and name == "out":
            start_own(name, kind)
    fetch("doc").wait()
    docs[0] = doc_ref[blocks - 1 : blocks, :]
    send(docs.at[0], docs.at[1], halo_send.at[2], halo_recv.at[2], z_next)
    for name, kind, lag in STREAMS:
        if lag == 0 and name != "out":
            start_own(name, kind)
    for name in fulls:
        at = pl.multiple_of(s * depth, depth)
        for k in range(3):
            mine_rows = fulls[name].at[k, pl.ds(at, depth), :]
            pltpu.make_async_copy(owns[name].at[:, pl.ds(k * third, third)], mine_rows, own_sem.at[0]).start()
    pltpu.make_async_copy(down_ref, dfull.at[0, 0], own_sem.at[0]).start()
    pltpu.make_async_copy(out_weight_ref, ofull.at[0, 0], own_sem.at[0]).start()
    for name in ("query", "key", "value", "sink"):
        fetch(name).wait()

    def column(row):
        return jnp.transpose(jnp.broadcast_to(row, (WINDOW, WINDOW)))

    def attend(b):
        first = b * WINDOW
        query = query_ref[first : first + WINDOW, :]
        query = jnp.concatenate([query[:, :HEAD_DIM], query[:, HEAD_DIM:]], axis=0)
        window = slice(first, first + 2 * WINDOW)
        scores = jnp.dot(query, keys[:, window], preferred_element_type=f32) * HEAD_DIM ** (-0.5)
        at_row = lax.broadcasted_iota(jnp.int32, (WINDOW, 2 * WINDOW), 0)
        at_col = lax.broadcasted_iota(jnp.int32, (WINDOW, 2 * WINDOW), 1)
        distance = at_row - at_col + WINDOW
        place_of_key = s * length + (first - WINDOW) + at_col
        own_doc = doc_ref[b : b + 1, :]
        mine_doc = column(own_doc)
        mine_doc = jnp.concatenate([mine_doc, mine_doc], axis=1)
        earlier = docs[1] if b == 0 else doc_ref[b - 1 : b, :]
        valid = (distance >= 0) & (distance < WINDOW) & (place_of_key >= 0)
        valid = valid & (mine_doc == jnp.concatenate([earlier, own_doc], axis=1))
        bias = jnp.where(valid, 0.0, masked_value)
        bias = jnp.concatenate([bias, bias], axis=0)
        scores = jnp.where(bias < 0.0, masked_value, scores)
        head = lax.broadcasted_iota(jnp.int32, (2 * WINDOW, 1), 0)
        sinks = jnp.where(head < WINDOW, sink_ref[0], sink_ref[1])
        top = jnp.maximum(jnp.max(scores, axis=-1, keepdims=True), sinks)
        weight = jnp.exp(scores - top)
        denom = jnp.sum(weight, axis=-1, keepdims=True) + jnp.exp(sinks - top)
        summed = lax.dot_general(
            weight.astype(bf16),
            values[:, window],
            (((1,), (1,)), ((), ())),
            preferred_element_type=f32,
        ) / denom
        mixed[first : first + WINDOW, :] = jnp.concatenate(
            [summed[:WINDOW], summed[WINDOW:]], axis=1
        ).astype(bf16)

    for b in range(1, blocks):
        attend(b)
    serve_until("out", 1)
    landed(keys.at[:, pl.ds(0, WINDOW)], halo_send.at[0], halo_recv.at[0], z_prev)
    landed(values.at[:, pl.ds(0, WINDOW)], halo_send.at[1], halo_recv.at[1], z_prev)
    landed(docs.at[1], halo_send.at[2], halo_recv.at[2], z_prev)
    attend(0)
    for d in range(n_tp):
        u = (d % 2) * n_x + d // 2
        heads[u * rows : (u + 1) * rows, :] = mixed[d * rows : (d + 1) * rows, :]
    arrived = gfull.at[0, pl.ds(0, 9 * depth + depth // 2), :]
    pltpu.make_async_copy(arrived, arrived, own_sem.at[0]).wait()
    for name in ("residual", "gain_mixed", "gain_before", "gain_after"):
        fetch(name).wait()

    def project(slot, at):
        right = jnp.concatenate([ofull[slot, side] for side in range(2)], axis=1)
        return jnp.dot(heads[pl.ds(at, half), :], right, preferred_element_type=f32)

    make, spread, pass_on, collect = summing(0, project, proj)
    for i in range(reach):
        serve_until("out", i + 1)
        make(i)
        if i >= 1:
            pass_on(i - 1)
        if i >= 2:
            collect(i - 2)
        serve(SERVE_RS[2] if i == reach - 1 else 1)
        spread(i)
        if i < reach - 1:
            serve_through(i + 1)
    serve(SERVE_RS[0])
    pass_on(reach - 1)
    collect(reach - 2)
    serve(SERVE_RS[1])
    collect(reach - 1)

    def scale_of(squares):
        return lax.rsqrt(squares / dim + epsilon)

    def normalise():
        squares = None
        for n in range(n_sp):
            v = proj[n].astype(bf16).astype(f32)
            part = jnp.sum(v * v, axis=-1, keepdims=True)
            squares = part if squares is None else squares + part
        scale = scale_of(squares)
        squares = None
        for n in range(n_sp):
            lanes = slice(n * width, (n + 1) * width)
            v = proj[n].astype(bf16).astype(f32)
            v = residual_ref[:, lanes].astype(f32) + v * scale * gain_mixed_ref[:, lanes]
            v = v.astype(bf16)
            after[:, lanes] = v
            v = v.astype(f32)
            part = jnp.sum(v * v, axis=-1, keepdims=True)
            squares = part if squares is None else squares + part
        scale = scale_of(squares)
        for n in range(n_sp):
            lanes = slice(n * width, (n + 1) * width)
            v = after[:, lanes].astype(f32)
            normed[:, lanes] = (v * scale * gain_before_ref[:, lanes]).astype(bf16)

    normalise()

    h_rows = rows // 2
    ag_at = {}

    def row_part(c, xx, h):
        return xn.at[pl.ds(pl.multiple_of(block_of(c, xx) + h * h_rows, h_rows), h_rows), :]

    def ag_send_to(key, src, dst, device):
        if key not in ag_at:
            ag_at[key] = len(ag_at)
        send(src, dst, ag_send.at[0], ag_recv.at[ag_at[key]], device)

    def ag_wait(key, dst):
        landed(dst, ag_send.at[0], ag_recv.at[ag_at[key]], partner)

    for h in range(2):
        src = normed.at[pl.ds(h * h_rows, h_rows), :]
        ag_send_to(("next", h), src, row_part(core, x, h), x_next)
        src = normed.at[pl.ds((1 - h) * h_rows, h_rows), :]
        ag_send_to(("prev", 1 - h), src, row_part(core, x, 1 - h), x_prev)
        src = normed.at[pl.ds(h * h_rows, h_rows), :]
        ag_send_to("partner", src, row_part(core, x, h), partner)
    xn[pl.ds(block_of(core, x), rows), :] = normed[...]

    def relay(h):
        for key, hh, xx, far, to in (("next", h, x - 1, 0, x_next), ("prev", 1 - h, x + 1, 1, x_prev)):
            here = row_part(core, xx, hh)
            ag_wait((key, hh), here)
            if hh == far:
                ag_send_to(("far", hh), here, here, to)
            ag_send_to("partner", here, here, partner)

    def relay_far(h):
        here = row_part(core, x + 2, h)
        ag_wait(("far", h), here)
        ag_send_to("partner", here, here, partner)

    serve(SERVE_AG[0])
    relay(0)
    serve(SERVE_AG[1])
    relay(1)
    serve(SERVE_AG[2])
    relay_far(0)
    relay_far(1)
    serve(SERVE_AG[3])
    ag_wait("partner", xn.at[pl.ds(block_of(other, 0), half), :])

    def units(k, b):
        piece = xn[b * half : (b + 1) * half, :]
        gate = jnp.dot(piece, gfull[k], preferred_element_type=f32)
        up = jnp.dot(piece, ufull[k], preferred_element_type=f32)
        hid[k, b * half : (b + 1) * half, :] = (gate / (1.0 + jnp.exp(-gate)) * up).astype(bf16)

    for turn, k in enumerate((mine, theirs, 1)):
        for name in fulls:
            if turn == 1:
                swapped(name)
            else:
                serve_until(name, reach, turn // 2)
        for b in range(2):
            units(k, b)
            serve(SERVE_UNITS)

    def lower(slot, at):
        total = None
        for k in range(3):
            right = jnp.concatenate(
                [dfull[slot, side, k * third : (k + 1) * third, :] for side in range(2)], axis=1
            )
            term = jnp.dot(hid[k, pl.ds(at, half), :], right, preferred_element_type=f32)
            total = term if total is None else total + term
        return total

    make, spread, pass_on, collect = summing(1, lower, ffn)
    for i in range(reach):
        if i >= 1:
            spread(i - 1)
        if i >= 3:
            pass_on(i - 3)
        if i >= 5:
            collect(i - 5)
        serve_until("down", i + 1)
        swapped("down", i + 1)
        make(i)
        if i >= 1:
            serve(1)
    pass_on(reach - 3)
    collect(reach - 5)
    spread(reach - 1)
    pass_on(reach - 2)
    collect(reach - 4)
    collect(reach - 3)
    pass_on(reach - 1)
    collect(reach - 2)
    collect(reach - 1)

    def finish():
        squares = None
        for n in range(n_sp):
            v = ffn[n].astype(bf16).astype(f32)
            part = jnp.sum(v * v, axis=-1, keepdims=True)
            squares = part if squares is None else squares + part
        scale = scale_of(squares)
        for n in range(n_sp):
            lanes = slice(n * width, (n + 1) * width)
            v = ffn[n].astype(bf16).astype(f32)
            out_ref[:, lanes] = (
                after[:, lanes].astype(f32) + 0.5 * (v * scale * gain_after_ref[:, lanes])
            ).astype(bf16)

    finish()

    def drain():
        trips = n_sp - 1
        shard = gfull.at[pl.ds(0, 2), pl.ds(0, trips * depth), :]
        swap = gfull.at[0, pl.ds(0, trips * depth), :]
        for i, name in enumerate(names):
            if name == "out":
                sent(gfull.at[0, pl.ds(0, trips * depth // 2), :], z_send.at[i])
            else:
                sent(shard, z_send.at[i])
                sent(swap, y_send.at[i])
        sent(xn.at[pl.ds(0, length - rows), :], ag_send.at[0])
        sent(pcs, pc_send.at[0])
        sent(raws, raw_send.at[0])
        sent(nbs, nb_send.at[0])
        tail = pl.ds(0, WINDOW)
        sent(keys.at[:, tail], halo_send.at[0])
        sent(values.at[:, tail], halo_send.at[1])
        sent(docs.at[0], halo_send.at[2])

    drain()


def per_device(
    queries,
    key_rows,
    value_rows,
    doc_ids,
    sink_logits,
    out_weight,
    residual,
    gain_mixed,
    gain_before,
    gain_after,
    gate_weight,
    up_weight,
    down_weight,
):
    n_sp, n_tp = lax.axis_size("sp"), lax.axis_size("tp")
    n_x, reach = n_tp // 2, n_sp // 2
    length = queries.shape[0]
    rows, dim = residual.shape
    depth, hidden = gate_weight.shape
    width = down_weight.shape[1]
    third = hidden // 3
    half = n_x * rows
    vmem = pl.BlockSpec(memory_space=pltpu.VMEM)
    hbm = pl.BlockSpec(memory_space=pltpu.HBM)
    dma = pltpu.SemaphoreType.DMA
    pieces = sum(PARTS.values())
    return pl.pallas_call(
        kernel,
        out_shape=jax.ShapeDtypeStruct((rows, dim), bf16),
        in_specs=[hbm] * 13,
        out_specs=vmem,
        scratch_shapes=[
            pltpu.VMEM((key_rows.shape[1], length + WINDOW), bf16),
            pltpu.VMEM((value_rows.shape[1], length + WINDOW), bf16),
            pltpu.VMEM((2, 1, WINDOW), jnp.int32),
            pltpu.VMEM(queries.shape, bf16),
            pltpu.VMEM(queries.shape, bf16),
            pltpu.VMEM((reach, 2, *out_weight.shape), bf16),
            pltpu.VMEM((3, n_sp * depth, third), bf16),
            pltpu.VMEM((3, n_sp * depth, third), bf16),
            pltpu.VMEM((reach, 2, hidden, width), bf16),
            pltpu.VMEM((n_sp, rows, width), f32),
            pltpu.VMEM((rows, dim), bf16),
            pltpu.VMEM((rows, dim), bf16),
            pltpu.VMEM((length, dim), bf16),
            pltpu.VMEM((3, length, third), bf16),
            pltpu.VMEM((reach, half, 2 * width), f32),
            pltpu.VMEM((2 * reach, half, 2 * width), bf16),
            pltpu.VMEM((2 * reach, half, 2 * width), bf16),
            pltpu.VMEM((2 * reach, 2, rows, width), bf16),
            pltpu.VMEM((2 * reach, 2, rows, width), bf16),
            pltpu.VMEM((2 * reach, 2, 2, rows, width), bf16),
            pltpu.VMEM((2 * reach, 2, 2, rows, width), bf16),
            pltpu.VMEM((n_sp, rows, width), f32),
            pltpu.VMEM((rows, dim), bf16),
            pltpu.VMEM(queries.shape, bf16),
            pltpu.VMEM((length // WINDOW, WINDOW), jnp.int32),
            pltpu.SMEM(sink_logits.shape, f32),
            pltpu.VMEM((1, dim), f32),
            pltpu.VMEM((1, dim), f32),
            pltpu.VMEM((1, dim), f32),
            dma((10,)),
            dma((3,)),
            dma((3,)),
            dma((4,)),
            dma((2 * reach * pieces,)),
            dma((3,)),
            dma((2 + reach,)),
            dma((1,)),
            dma((7,)),
            dma((1,)),
            dma((reach,)),
            dma((1,)),
            dma((reach,)),
            dma((1,)),
            dma((reach,)),
        ],
        compiler_params=pltpu.CompilerParams(
            collective_id=0, has_side_effects=True, vmem_limit_bytes=44 * 1024 * 1024
        ),
    )(
        *(
            pltpu.with_memory_space_constraint(array, pltpu.HBM)
            for array in (
                queries,
                key_rows.T,
                value_rows.T,
                doc_ids.reshape(-1, WINDOW),
                sink_logits,
                residual,
                gain_mixed.reshape(1, -1),
                gain_before.reshape(1, -1),
                gain_after.reshape(1, -1),
                out_weight,
                gate_weight,
                up_weight,
                down_weight,
            )
        )
    )


def solution(mesh):
    return jax.shard_map(
        per_device,
        mesh=mesh,
        in_specs=(
            P(("grp", "sp"), "tp"),
            P(("grp", "sp"), "tp"),
            P(("grp", "sp"), "tp"),
            P(("grp", "sp")),
            P("tp"),
            P("tp", "sp"),
            P(("grp", "sp", "tp"), None),
            P(),
            P(),
            P(),
            P("sp", "tp"),
            P("sp", "tp"),
            P("tp", "sp"),
        ),
        out_specs=P(("grp", "sp", "tp"), None),
        check_vma=False,
    )
```
